512 devices in a mesh: ep: 32 (over z, x), tp: 16 (over y, core).
Axes of the slice: x: 4, y: 8, z: 8, core: 2. Of those that a mesh axis runs over, the one named last changes fastest.
Arguments:
- mixer_in: bfloat16 [4096, 2048], P('ep'), may hold values from -6 to 6
- mixer_gain: float32 [2048], replicated, may hold values from 0.1 to 1.9
- w_value: bfloat16 [2048, 1536], P(None, 'tp'), may hold values from -0.125 to 0.125
- w_gate: bfloat16 [2048, 1536], P(None, 'tp'), may hold values from -0.125 to 0.125
- w_taps: float32 [31, 1536], P(None, 'tp'), may hold values from -3 to 3
- channel_gain: float32 [1536], P('tp'), may hold values from 0.1 to 1.9
- w_output: bfloat16 [1536, 2048], P('tp'), may hold values from -0.15625 to 0.15625
- expert_in: bfloat16 [4096, 2048], P('ep'), may hold values from -6 to 6
- expert_gain: float32 [2048], replicated, may hold values from 0 to 8
- route_experts: int32 [4096, 4], P('ep'), may hold values from 0 to 31, all different within a row; in each aligned block of 128 rows (0 to 127, 128 to 255, ...) at most 32 rows name the same one
- route_scores: float32 [4096, 4], P('ep'), may hold values from -6 to 6
- expert_gate: bfloat16 [32, 2048, 2048], P('ep', None, 'tp'), may hold values from -0.125 to 0.125
- expert_up: bfloat16 [32, 2048, 2048], P('ep', None, 'tp'), may hold values from -0.125 to 0.125
- expert_down: bfloat16 [32, 2048, 2048], P('ep', 'tp'), may hold values from -0.125 to 0.125
Outputs:
- mixer_out: bfloat16 [4096, 2048], P('ep')
- expert_out: bfloat16 [4096, 2048], P('ep')
The draws below stay inside these ranges and needn't reach their ends.
Inputs may be any that keep to these rules, and one draw needn't show every extreme that they name: `route_experts`: each row names 4 different experts. In each aligned block of 128 rows (the rows of one index of ep) no expert is named more than 32 times, a bound that some block reaches.
All inputs are finite; a program needn't handle non-finite values.
Results may differ from the reference program's by a relative error of at most 0.02.
Values may be sent and summed in bfloat16 or wider, within the bound.
A program may use at most 64 MiB of HBM per device.

```python
import math
import jax
import jax.numpy as jnp
import numpy as np
from jax import lax

D = 2048
CONV_CH = 1536
CONV_W = 31
FF = 2048
TOP_K = 4
TOK = 128
EXPERTS = 32
SEQ = 4096
CAP = 32
CH_DEV = 96
FF_DEV = 128
N_EP = 32


def draw_w_taps(key, part):
    base_key, factor_key = jax.random.split(jax.random.fold_in(key, 17))
    base_taps = jnp.clip(jax.random.normal(base_key, (CONV_W, CONV_CH), jnp.float32), -4.0, 4.0) * CONV_W ** (-0.5)
    factors = jnp.exp(jax.random.uniform(factor_key, (CONV_CH // CH_DEV,), jnp.float32, -math.log(3.0), math.log(3.0)))
    return base_taps * jnp.repeat(factors, CH_DEV)[None, :]


def draw_expert_gain(key, part):
    noise = jnp.clip(jax.random.normal(jax.random.fold_in(key, 29), (D,), jnp.float32), -3.0, 3.0)
    gain_values = 1.0 + 0.18 * noise
    return gain_values


def steps_of(rng, dims, cuts, low, largest):
    def one(dim, parts):
        steps = jax.random.uniform(jax.random.fold_in(jax.random.fold_in(rng, 6), dim), (parts,), jnp.float32, low / len(cuts), largest / len(cuts))
        return jnp.repeat(jnp.exp(steps), dims[dim] // parts).reshape((-1,) + (1,) * (len(dims) - dim - 1))

    level = one(*cuts[0])
    for cut in cuts[1:]:
        level = level * one(*cut)
    return level


def assign_block(key, own, number, rows, count, top, reach, skew):
    sequence = jax.random.permutation(key, count)
    heavy_load, ordinary = portions_of(count, rows * top, reach, skew, True), portions_of(count, rows * top, reach, skew, False)
    places = jnp.arange(count)

    def named(sizes, rotation):
        used = int((sizes > 0).sum())
        fixed = max(1, used // 4)
        moved = fixed + (places - fixed + rotation * (used - fixed)) % max(1, count - fixed)
        return jnp.zeros((count,), jnp.int32).at[sequence[jnp.where(places < fixed, places, moved)]].set(jnp.asarray(sizes, jnp.int32))

    sizes = jnp.where(number % 4 == 0, named(heavy_load, number // 4), named(ordinary, number - number // 4 - 1))
    mixed = jax.random.permutation(jax.random.fold_in(own, 3), count)
    giver, receiver = mixed[0:count // 2 * 2:2], mixed[1:count // 2 * 2:2]
    room = jnp.minimum(sizes[giver] - 1, reach - sizes[receiver]) // 2
    room = jnp.where((giver == sequence[0]) | (receiver == sequence[0]) | (sizes[receiver] == 0), 0, jnp.maximum(room, 0))
    moved = jax.random.randint(jax.random.fold_in(own, 4), (count // 2,), 0, 1 << 20) % (room + 1)
    sizes = sizes.at[giver].add(-moved).at[receiver].add(moved)
    members = jnp.searchsorted(jnp.cumsum(sizes), jnp.arange(rows * top), side="right").astype(jnp.int32)
    grid = members.reshape(top, rows).T
    grid = grid[jax.random.permutation(jax.random.fold_in(own, 1), rows)]
    rotation = jax.random.randint(jax.random.fold_in(own, 2), (rows, 1), 0, top)
    return jnp.take_along_axis(grid, (jnp.arange(top)[None, :] + rotation) % top, axis=1)


def portions_of(count, total, most, slope, full):
    weights = [(1 << 20) // math.isqrt(rank ** slope) + 1 for rank in range(1, count + 1)]
    largest = most if full else min(most, max(-(-total // count), total * weights[0] // sum(weights)))
    least = 1 if total - largest >= count - 1 else 0
    given, spare = [largest] + [least] * (count - 1), total - largest - least * (count - 1)
    while spare > 0:
        candidates = [i for i in range(1, count) if given[i] < largest] or [i for i in range(1, count) if given[i] < most]
        pool, budget = sum([weights[i] for i in candidates]), spare
        for i in candidates:
            addition = min(most - given[i], max(1, budget * weights[i] // pool), spare)
            given[i] = given[i] + addition
            spare = spare - addition
    return np.array(given)


def centred(key, shape, scale, reach, cuts=(), kind=jnp.bfloat16):
    factor_of = steps_of(key, shape, cuts, -0.22, 0.18) if cuts else 1.0
    drawn = jax.random.normal(key, shape, jnp.float32) * scale * factor_of
    return jnp.minimum(jnp.maximum(drawn, -reach), reach).astype(kind)


def setup_inputs(seed: int = 0) -> dict:
    streams_of = jax.random.split(jax.random.key(seed), 15)
    mixer_in = centred(streams_of[0], (SEQ, D), 1.0, 6.0, ((0, 32),))
    mixer_gain = jnp.clip(1.0 + 0.18 * jax.random.normal(streams_of[1], (D,), jnp.float32), 0.1, 1.9)
    w_value = centred(streams_of[2], (D, CONV_CH), D ** -0.5, 0.125, ((1, 16),))
    w_gate = centred(streams_of[3], (D, CONV_CH), D ** -0.5, 0.125, ((1, 16),))
    w_taps = draw_w_taps(jax.random.fold_in(streams_of[14], 71), 0)
    channel_gain = jnp.clip(1.0 + 0.18 * jax.random.normal(streams_of[5], (CONV_CH,), jnp.float32), 0.1, 1.9)
    w_output = centred(streams_of[6], (CONV_CH, D), CONV_CH ** -0.5, 0.15625, ((0, 16),))
    expert_in = centred(streams_of[7], (SEQ, D), 1.0, 6.0, ((0, 32),))
    expert_gain = draw_expert_gain(jax.random.fold_in(streams_of[14], 71), 0)
    route_experts_keys = jax.random.split(jax.random.fold_in(streams_of[9], 1), SEQ // TOK)
    route_experts_turns = jax.random.permutation(jax.random.fold_in(streams_of[9], 3), SEQ // TOK)
    route_experts = jax.vmap(lambda own, number: assign_block(jax.random.fold_in(streams_of[9], 2), own, number, TOK, EXPERTS, TOP_K, CAP, 1))(route_experts_keys, route_experts_turns).reshape((SEQ, TOP_K))
    route_scores = centred(streams_of[10], (SEQ, TOP_K), 1.0, 6.0, ((0, 32),), jnp.float32)
    expert_gate = centred(streams_of[11], (EXPERTS, D, FF), D ** -0.5, 0.125, ((0, 32), (2, 16)))
    expert_up = centred(streams_of[12], (EXPERTS, D, FF), D ** -0.5, 0.125, ((0, 32), (2, 16)))
    expert_down = centred(streams_of[13], (EXPERTS, FF, D), FF ** -0.5, 0.125, ((0, 32), (1, 16)))
    return {"mixer_in": mixer_in, "mixer_gain": mixer_gain, "w_value": w_value, "w_gate": w_gate, "w_taps": w_taps, "channel_gain": channel_gain, "w_output": w_output, "expert_in": expert_in, "expert_gain": expert_gain, "route_experts": route_experts, "route_scores": route_scores, "expert_gate": expert_gate, "expert_up": expert_up, "expert_down": expert_down}


epsilon = 1e-05
clamp_limit = 7.0
swish_slope = 1.702

def row_norm(inputs, gains):
    widened = inputs.astype(jnp.float32)
    row_mean = lax.optimization_barrier(jnp.mean(widened, axis=-1, keepdims=True))
    row_var = lax.optimization_barrier(jnp.mean(jnp.square(widened - row_mean), axis=-1, keepdims=True))
    return (widened - row_mean) * lax.rsqrt(row_var + epsilon) * gains

def mixer_half(mixer_in, mixer_gain, w_value, w_gate, w_taps, channel_gain, w_output):
    normed = row_norm(mixer_in, mixer_gain).astype(jnp.bfloat16)
    values = jnp.dot(normed, w_value, preferred_element_type=jnp.float32)
    gate_pre = jnp.dot(normed, w_gate, preferred_element_type=jnp.float32)
    gated_values = (values * jax.nn.sigmoid(gate_pre)).astype(jnp.bfloat16)
    extended = jnp.concatenate([jnp.zeros((CONV_W - 1, CONV_CH), jnp.bfloat16), gated_values], axis=0)
    conv_out = jnp.zeros((SEQ, CONV_CH), jnp.float32)
    for offset in range(CONV_W):
        conv_out = conv_out + extended[offset:offset + SEQ].astype(jnp.float32) * w_taps[offset]
    row_mean = lax.optimization_barrier(jnp.sum(conv_out, axis=1, keepdims=True)) / CONV_CH
    row_var = lax.optimization_barrier(jnp.sum(conv_out * conv_out, axis=1, keepdims=True)) / CONV_CH - row_mean * row_mean
    activated = jax.nn.silu((conv_out - row_mean) * lax.rsqrt(row_var + epsilon) * channel_gain).astype(jnp.bfloat16)
    summed = jnp.zeros((SEQ, D), jnp.float32)
    for block_index in range(CONV_CH // CH_DEV):
        first_col = block_index * CH_DEV
        block_term = jnp.dot(activated[:, first_col:first_col + CH_DEV], w_output[first_col:first_col + CH_DEV], preferred_element_type=jnp.float32)
        summed = summed + lax.optimization_barrier(block_term.astype(jnp.bfloat16)).astype(jnp.float32)
    return summed.astype(jnp.bfloat16)

def expert_half(expert_in, expert_gain, route_experts, route_scores, expert_gate, expert_up, expert_down):
    normed = row_norm(expert_in, expert_gain).astype(jnp.bfloat16)
    raised = jnp.exp(route_scores)
    route_weights = raised / lax.optimization_barrier(jnp.sum(raised, axis=1, keepdims=True))
    chosen = route_experts.reshape(N_EP, TOK * TOP_K).astype(jnp.int32)
    onehot = (chosen[:, :, None] == jnp.arange(EXPERTS, dtype=jnp.int32)[None, None, :]).astype(jnp.int32)
    slot_index = lax.optimization_barrier(jnp.sum((jnp.cumsum(onehot, axis=1) - onehot) * onehot, axis=2)).astype(jnp.int32)
    source = jnp.arange(N_EP, dtype=jnp.int32)[:, None]
    owner_row = (source * TOK + jnp.arange(TOK * TOP_K, dtype=jnp.int32)[None, :] // TOP_K).astype(jnp.int32)
    placed = ((chosen * N_EP + source) * CAP + slot_index).reshape(-1).astype(jnp.int32)
    slot_table = jnp.full((EXPERTS * N_EP * CAP,), SEQ, jnp.int32).at[placed].set(owner_row.reshape(-1))
    padded = jnp.concatenate([normed, jnp.zeros((1, D), jnp.bfloat16)], axis=0)

    def one_expert(operands):
        table_rows, gate_w, up_w, down_w = operands
        gathered = padded[table_rows.astype(jnp.int32)]
        gate_pre = jnp.minimum(jnp.dot(gathered, gate_w, preferred_element_type=jnp.float32), clamp_limit)
        up_pre = jnp.clip(jnp.dot(gathered, up_w, preferred_element_type=jnp.float32), -clamp_limit, clamp_limit)
        hidden = ((up_pre + 1.0) * gate_pre * jax.nn.sigmoid(swish_slope * gate_pre)).astype(jnp.bfloat16)
        summed = jnp.zeros((N_EP * CAP, D), jnp.float32)
        for block_index in range(FF // FF_DEV):
            first_col = block_index * FF_DEV
            block_term = jnp.dot(hidden[:, first_col:first_col + FF_DEV], down_w[first_col:first_col + FF_DEV], preferred_element_type=jnp.float32)
            summed = summed + lax.optimization_barrier(block_term.astype(jnp.bfloat16)).astype(jnp.float32)
        return summed.astype(jnp.bfloat16)
    expert_rows = lax.map(one_expert, (slot_table.reshape(EXPERTS, N_EP * CAP), expert_gate, expert_up, expert_down))
    picked = expert_rows.reshape(EXPERTS * N_EP * CAP, D)[placed].astype(jnp.float32).reshape(SEQ, TOP_K, D)
    return lax.optimization_barrier(jnp.sum(picked * route_weights[:, :, None], axis=1)).astype(jnp.bfloat16)

def reference(mixer_in, mixer_gain, w_value, w_gate, w_taps, channel_gain, w_output, expert_in, expert_gain, route_experts, route_scores, expert_gate, expert_up, expert_down):
    mixer_out = mixer_half(mixer_in, mixer_gain, w_value, w_gate, w_taps, channel_gain, w_output)
    expert_out = expert_half(expert_in, expert_gain, route_experts, route_scores, expert_gate, expert_up, expert_down)
    return (mixer_out, expert_out)
```

```python
import functools

import jax
import jax.numpy as jnp
from jax import lax
from jax.experimental import pallas as pl
from jax.experimental.pallas import tpu as pltpu
from jax.sharding import Mesh
from jax.sharding import PartitionSpec as P

CONV_CH = 1536
CONV_W = 31
EP = ("z", "x")
TP = ("y", "c")
NZ, NX, NY = 8, 4, 8
SLOTS = 32
FAR = NY // 2

epsilon = 1e-05
clamp_limit = 7.0
swish_slope = 1.702

VM = pl.BlockSpec(memory_space=pltpu.VMEM)
ANY = pl.BlockSpec(memory_space=pl.ANY)
DMA = pltpu.SemaphoreType.DMA


def shift_of(y, c, j):
    m = 2 * c + j
    return (2 * m + 1 - y // 4) % NZ, (y % 4 + m) % NX


def reach(way, j):
    return FAR if way == j else FAR - 1


def put(src, dst, sent, landed, **device):
    return pltpu.make_async_remote_copy(
        src_ref=src,
        dst_ref=dst,
        send_sem=sent,
        recv_sem=landed,
        device_id=device,
        device_id_type=pl.DeviceIdType.MESH,
    )


def greet(barrier, **device):
    pl.semaphore_signal(barrier, inc=1, device_id=device, device_id_type=pl.DeviceIdType.MESH)


def place():
    return tuple(lax.axis_index(a) for a in ("z", "x", "y", "c"))


def greet_shifts(barrier, z, x, y, c):
    itself = jnp.logical_and(y == 4, c == 0)
    for j in range(2):
        dz, dx = shift_of(y, c, j)

        def both():
            greet(barrier, z=(z + dz) % NZ, x=(x + dx) % NX)
            greet(barrier, z=(z + NZ - dz) % NZ, x=(x + NX - dx) % NX)

        if j == 0:
            pl.when(jnp.logical_not(itself))(both)
        else:
            both()
    return itself


def wait_greets(barrier, itself, others):
    pl.semaphore_wait(barrier, jnp.where(itself, others + 2, others + 4))


def dispatch_kernel(
    send, halo_in, gate_hbm, up_hbm, hidden, halo_out, rows, weights,
    w_sem, a_sent, a_here, local_sem, h_sent, h_here, hop_sent, hop_here,
    own_sent, own_here, rel_sent, rel_here,
):
    z, x, y, c = place()
    other = 1 - c
    sides = ((y + 1) % NY, (y + NY - 1) % NY)
    block = z * NX + x
    after = (block + 1) % (NZ * NX)
    before = (block + NZ * NX - 1) % (NZ * NX)

    barrier = pltpu.get_barrier_semaphore()
    itself = greet_shifts(barrier, z, x, y, c)
    greet(barrier, y=sides[0])
    greet(barrier, y=sides[1])
    greet(barrier, c=other)
    greet(barrier, z=after // NX, x=after % NX)
    greet(barrier, z=before // NX, x=before % NX)
    gate_copy = pltpu.make_async_copy(gate_hbm.at[0], weights.at[:, pl.ds(0, 128)], w_sem.at[0])
    up_copy = pltpu.make_async_copy(up_hbm.at[0], weights.at[:, pl.ds(128, 128)], w_sem.at[1])
    gate_copy.start()
    up_copy.start()
    wait_greets(barrier, itself, 5)

    def shifted(j):
        dz, dx = shift_of(y, c, j)
        return put(
            send.at[j], rows.at[c, y, j], a_sent.at[j], a_here.at[j],
            z=(z + dz) % NZ, x=(x + dx) % NX,
        )

    stays = pltpu.make_async_copy(send.at[0], rows.at[c, y, 0], local_sem)

    @pl.when(itself)
    def _():
        stays.start()

    @pl.when(jnp.logical_not(itself))
    def _():
        shifted(0).start()

    shifted(1).start()
    halo = put(halo_in, halo_out, h_sent, h_here, z=after // NX, x=after % NX)
    halo.start()

    def origin(k, way):
        return (y + NY - k) % NY if way == 0 else (y + k) % NY

    def hop(k, j, way):
        piece = rows.at[c, origin(k, way), j]
        return put(piece, piece, hop_sent.at[way, k, j], hop_here.at[way, k, j], y=sides[way])

    def own(j):
        piece = rows.at[c, y, j]
        return put(piece, piece, own_sent.at[j], own_here.at[j], c=other)

    def relay(k, j, way):
        piece = rows.at[c, origin(k + 1, way), j]
        return put(piece, piece, rel_sent.at[way, k, j], rel_here.at[way, k, j], c=other)

    def product(core, source):
        inputs = rows[core, source].reshape(2 * SLOTS, 2048)
        both = jnp.dot(inputs, weights[...], preferred_element_type=jnp.float32)
        gate = jnp.minimum(both[:, :128], clamp_limit)
        up = jnp.clip(both[:, 128:], -clamp_limit, clamp_limit)
        hidden[core, source] = (
            (up + 1.0) * gate * jax.nn.sigmoid(swish_slope * gate)
        ).astype(jnp.bfloat16)

    for j in range(2):
        if j == 0:

            @pl.when(itself)
            def _():
                stays.wait()

            @pl.when(jnp.logical_not(itself))
            def _():
                shifted(0).wait()
        else:
            shifted(1).wait()
        for way in range(2):
            hop(0, j, way).start()
        own(j).start()
    gate_copy.wait()
    up_copy.wait()
    product(c, y)
    for j in range(2):
        own(j).wait()
    product(other, y)
    for k in range(FAR):
        for j in range(2):
            for way in range(2):
                if k < reach(way, j):
                    hop(k, j, way).wait_recv()
                    if k + 1 < reach(way, j):
                        hop(k + 1, j, way).start()
                    relay(k, j, way).start()
        ways = (0, 1) if k < FAR - 1 else (0,)
        for way in ways:
            product(c, origin(k + 1, way))
        for j in range(2):
            for way in range(2):
                if k < reach(way, j):
                    relay(k, j, way).wait_recv()
        for way in ways:
            product(other, origin(k + 1, way))
    halo.wait()
    for k in range(FAR):
        for j in range(2):
            for way in range(2):
                if k < reach(way, j):
                    hop(k, j, way).wait_send()
                    relay(k, j, way).wait_send()


def dispatch(send, halo_in, gate_w, up_w):
    return pl.pallas_call(
        dispatch_kernel,
        out_shape=(
            jax.ShapeDtypeStruct((2, NY, 2 * SLOTS, 128), jnp.bfloat16),
            jax.ShapeDtypeStruct((32, 128), jnp.bfloat16),
        ),
        in_specs=[VM, VM, ANY, ANY],
        out_specs=(VM, VM),
        scratch_shapes=[
            pltpu.VMEM((2, NY, 2, SLOTS, 2048), jnp.bfloat16),
            pltpu.VMEM((2048, 256), jnp.bfloat16),
            DMA((2,)),
            DMA((2,)),
            DMA((2,)),
            DMA,
            DMA,
            DMA,
            DMA((2, FAR, 2)),
            DMA((2, FAR, 2)),
            DMA((2,)),
            DMA((2,)),
            DMA((2, FAR, 2)),
            DMA((2, FAR, 2)),
        ],
        compiler_params=pltpu.CompilerParams(
            collective_id=0, has_side_effects=True, vmem_limit_bytes=24 << 20
        ),
        name="dispatch",
    )(send, halo_in, gate_w, up_w)


def combine_kernel(
    hidden, down, stats, returned, stats_out, given, taken, chain_in, chain_out, mine,
    final, pair, pair_sum, stats_all, give_sent, give_here, hop_sent, hop_here, r_sent, r_here,
    local_sem, p_sent, p_here, s_sent, s_here,
):
    z, x, y, c = place()
    other = 1 - c
    sides = ((y + 1) % NY, (y + NY - 1) % NY)
    barrier = pltpu.get_barrier_semaphore()
    itself = greet_shifts(barrier, z, x, y, c)
    greet(barrier, c=other)
    for i in range(1, NY):
        greet(barrier, y=(y + i) % NY)

    def away(m, way):
        return (y + m) % NY if way == 0 else (y + NY - m) % NY

    order = [(FAR, 0)] + [(m, way) for m in range(FAR - 1, 0, -1) for way in range(2)] + [(0, 0)]

    def gift(i):
        dest = away(*order[i])
        return put(given.at[dest], taken.at[dest], give_sent.at[i], give_here.at[i], c=other)

    def give(i):
        dest = away(*order[i])

        def columns(n, _):
            at = pl.ds(pl.multiple_of(n * 512, 512), 512)
            given[dest, :, at] = jnp.dot(
                hidden[other, dest], down[0, :, at], preferred_element_type=jnp.float32
            ).astype(jnp.bfloat16)
            return 0

        lax.fori_loop(0, 4, columns, 0)
        gift(i).start()

    def add_up(i, slot):
        dest = away(*order[i])
        gift(i).wait_recv()

        def columns(n, _):
            at = pl.ds(pl.multiple_of(n * 512, 512), 512)
            mine[slot, :, at] = jnp.dot(
                hidden[c, dest], down[0, :, at], preferred_element_type=jnp.float32
            ) + taken[dest, :, at].astype(jnp.float32)
            return 0

        lax.fori_loop(0, 4, columns, 0)

    def hop(m, j, way):
        return put(
            chain_out.at[way, m - 1, j], chain_in.at[way, m - 1, j],
            hop_sent.at[way, m - 1, j], hop_here.at[way, m - 1, j], y=sides[way],
        )

    def pass_on(m, j, way, slot):
        total = mine[slot, j * SLOTS : (j + 1) * SLOTS]
        if m < reach(way, j):
            hop(m + 1, j, way).wait_recv()
            total = total + chain_in[way, m, j].astype(jnp.float32)
        chain_out[way, m - 1, j] = total.astype(jnp.bfloat16)
        hop(m, j, way).start()

    def swap():
        return put(stats, pair, p_sent, p_here, c=other)

    def spread(i):
        return put(
            pair_sum, stats_all.at[y], s_sent.at[i], s_here.at[i], y=(y + i) % NY
        )

    dest = away(*order[0])

    def first(n, _):
        at = pl.ds(pl.multiple_of(n * 512, 512), 512)
        given[dest, :, at] = jnp.dot(
            hidden[other, dest], down[0, :, at], preferred_element_type=jnp.float32
        ).astype(jnp.bfloat16)
        return 0

    lax.fori_loop(0, 4, first, 0)
    wait_greets(barrier, itself, NY)
    gift(0).start()
    swap().start()
    give(1)
    give(2)
    add_up(0, 0)
    pass_on(FAR, 0, 0, 0)
    pass_on(FAR, 1, 1, 0)
    for m in range(FAR - 1, 0, -1):
        i = 1 + 2 * (FAR - 1 - m)
        give(i + 2)
        if m > 1:
            give(i + 3)
        add_up(i, 0)
        add_up(i + 1, 1)
        for turn in range(2):
            for way in range(2):
                pass_on(m, 1 - way if turn == 0 else way, way, way)
        if m == FAR - 1:
            swap().wait()
            pair_sum[...] = stats[...] + pair[...]
            for i in range(1, NY):
                spread(i).start()
    add_up(len(order) - 1, 0)
    total = pair_sum[...]
    for i in range(1, NY):
        spread(i).wait()
        total = total + stats_all[(y + NY - i) % NY]
    stats_out[...] = total

    def goes_back(j):
        dz, dx = shift_of(y, c, j)
        return put(
            final.at[j], returned.at[j], r_sent.at[j], r_here.at[j],
            z=(z + NZ - dz) % NZ, x=(x + NX - dx) % NX,
        )

    stays = pltpu.make_async_copy(final.at[0], returned.at[0], local_sem)
    for j in range(2):
        hop(1, j, 0).wait_recv()
        hop(1, j, 1).wait_recv()
        final[j] = (
            mine[0, j * SLOTS : (j + 1) * SLOTS]
            + chain_in[0, 0, j].astype(jnp.float32)
            + chain_in[1, 0, j].astype(jnp.float32)
        ).astype(jnp.bfloat16)
        if j == 0:

            @pl.when(itself)
            def _():
                stays.start()

            @pl.when(jnp.logical_not(itself))
            def _():
                goes_back(0).start()
        else:
            goes_back(1).start()
    for i in range(len(order)):
        gift(i).wait_send()
    for m in range(1, FAR + 1):
        for j in range(2):
            for way in range(2):
                if m <= reach(way, j):
                    hop(m, j, way).wait_send()

    @pl.when(itself)
    def _():
        stays.wait()

    @pl.when(jnp.logical_not(itself))
    def _():
        goes_back(0).wait()

    goes_back(1).wait()


def combine(hidden, down_w, stats):
    return pl.pallas_call(
        combine_kernel,
        out_shape=(
            jax.ShapeDtypeStruct((2, SLOTS, 2048), jnp.bfloat16),
            jax.ShapeDtypeStruct((8, 128), jnp.float32),
        ),
        in_specs=[VM, VM, VM],
        out_specs=(VM, VM),
        scratch_shapes=[
            pltpu.VMEM((NY, 2 * SLOTS, 2048), jnp.bfloat16),
            pltpu.VMEM((NY, 2 * SLOTS, 2048), jnp.bfloat16),
            pltpu.VMEM((2, FAR, 2, SLOTS, 2048), jnp.bfloat16),
            pltpu.VMEM((2, FAR, 2, SLOTS, 2048), jnp.bfloat16),
            pltpu.VMEM((2, 2 * SLOTS, 2048), jnp.float32),
            pltpu.VMEM((2, SLOTS, 2048), jnp.bfloat16),
            pltpu.VMEM((8, 128), jnp.float32),
            pltpu.VMEM((8, 128), jnp.float32),
            pltpu.VMEM((NY, 8, 128), jnp.float32),
            DMA((2 * FAR,)),
            DMA((2 * FAR,)),
            DMA((2, FAR, 2)),
            DMA((2, FAR, 2)),
            DMA((2,)),
            DMA((2,)),
            DMA,
            DMA,
            DMA,
            DMA((NY,)),
            DMA((NY,)),
        ],
        compiler_params=pltpu.CompilerParams(
            collective_id=1, has_side_effects=True, vmem_limit_bytes=32 << 20
        ),
        name="combine",
    )(hidden, down_w, stats)


ROWS = 16
HALF = 1024


def total_kernel(
    part_m, part_e, out_m, out_e, taken, chain_in, chain_out,
    give_sent, give_here, hop_sent, hop_here, ring_sent, ring_here,
    own_sent, own_here, rel_sent, rel_here,
):
    z, x, y, c = place()
    other = 1 - c
    sides = ((y + 1) % NY, (y + NY - 1) % NY)
    parts, outs = (part_m, part_e), (out_m, out_e)
    mine = pl.ds(pl.multiple_of(c * HALF, HALF), HALF)
    theirs = pl.ds(pl.multiple_of(other * HALF, HALF), HALF)
    barrier = pltpu.get_barrier_semaphore()
    greet(barrier, y=sides[0])
    greet(barrier, y=sides[1])
    greet(barrier, c=other)
    pl.semaphore_wait(barrier, 3)

    def away(m, way):
        return (y + m) % NY if way == 0 else (y + NY - m) % NY

    def gift(j):
        return put(
            parts[j].at[:, :, theirs], taken.at[j], give_sent.at[j], give_here.at[j], c=other
        )

    for j in range(2):
        gift(j).start()

    def own(j, dest):
        return parts[j][dest, :, mine].astype(jnp.float32) + taken[j, dest].astype(jnp.float32)

    def hop(m, j, way):
        return put(
            chain_out.at[way, m - 1, j], chain_in.at[way, m - 1, j],
            hop_sent.at[way, m - 1, j], hop_here.at[way, m - 1, j], y=sides[way],
        )

    for j in range(2):
        gift(j).wait_recv()
    for m in range(FAR, 0, -1):
        for j in range(2):
            for way in range(2):
                if m <= reach(way, j):
                    total = own(j, away(m, way))
                    if m < reach(way, j):
                        hop(m + 1, j, way).wait_recv()
                        total = total + chain_in[way, m, j].astype(jnp.float32)
                    chain_out[way, m - 1, j] = total.astype(jnp.bfloat16)
                    hop(m, j, way).start()

    def origin(k, way):
        return (y + NY - k) % NY if way == 0 else (y + k) % NY

    def ring(k, j, way):
        piece = outs[j].at[origin(k, way), :, mine]
        return put(piece, piece, ring_sent.at[way, k, j], ring_here.at[way, k, j], y=sides[way])

    def swap(j):
        piece = outs[j].at[y, :, mine]
        return put(piece, piece, own_sent.at[j], own_here.at[j], c=other)

    def relay(k, j, way):
        piece = outs[j].at[origin(k + 1, way), :, mine]
        return put(piece, piece, rel_sent.at[way, k, j], rel_here.at[way, k, j], c=other)

    for j in range(2):
        hop(1, j, 0).wait_recv()
        hop(1, j, 1).wait_recv()
        outs[j][y, :, mine] = (
            own(j, y)
            + chain_in[0, 0, j].astype(jnp.float32)
            + chain_in[1, 0, j].astype(jnp.float32)
        ).astype(jnp.bfloat16)
        for way in range(2):
            ring(0, j, way).start()
        swap(j).start()
    for k in range(FAR):
        for j in range(2):
            for way in range(2):
                if k < reach(way, j):
                    ring(k, j, way).wait_recv()
                    if k + 1 < reach(way, j):
                        ring(k + 1, j, way).start()
                    relay(k, j, way).start()
    for j in range(2):
        gift(j).wait_send()
        swap(j).wait()
        for k in range(FAR):
            for way in range(2):
                if k < reach(way, j):
                    hop(k + 1, j, way).wait_send()
                    ring(k, j, way).wait_send()
                    relay(k, j, way).wait()


def total_over_tp(part_m, part_e):
    shape = (NY, ROWS, 2048)
    out_m, out_e = pl.pallas_call(
        total_kernel,
        out_shape=(jax.ShapeDtypeStruct(shape, jnp.bfloat16),) * 2,
        in_specs=[VM, VM],
        out_specs=(VM, VM),
        scratch_shapes=[
            pltpu.VMEM((2, NY, ROWS, HALF), jnp.bfloat16),
            pltpu.VMEM((2, FAR, 2, ROWS, HALF), jnp.bfloat16),
            pltpu.VMEM((2, FAR, 2, ROWS, HALF), jnp.bfloat16),
            DMA((2,)),
            DMA((2,)),
            DMA((2, FAR, 2)),
            DMA((2, FAR, 2)),
            DMA((2, FAR, 2)),
            DMA((2, FAR, 2)),
            DMA((2,)),
            DMA((2,)),
            DMA((2, FAR, 2)),
            DMA((2, FAR, 2)),
        ],
        compiler_params=pltpu.CompilerParams(
            collective_id=2, has_side_effects=True, vmem_limit_bytes=16 << 20
        ),
        name="total",
    )(part_m.reshape(shape), part_e.reshape(shape))
    return out_m.reshape(-1, 2048), out_e.reshape(-1, 2048)


def row_norm(inputs, gains):
    widened = inputs.astype(jnp.float32)
    row_mean = jnp.mean(widened, axis=-1, keepdims=True)
    row_var = jnp.mean(jnp.square(widened - row_mean), axis=-1, keepdims=True)
    return (widened - row_mean) * lax.rsqrt(row_var + epsilon) * gains


def local(
    mixer_in,
    mixer_gain,
    w_value,
    w_gate,
    w_taps,
    channel_gain,
    w_output,
    expert_in,
    expert_gain,
    route_experts,
    route_scores,
    expert_gate,
    expert_up,
    expert_down,
):
    z, x, y, c = place()
    tokens = expert_in.shape[0]

    normed = row_norm(mixer_in, mixer_gain).astype(jnp.bfloat16)
    values = jnp.dot(normed, w_value, preferred_element_type=jnp.float32)
    gate_pre = jnp.dot(normed, w_gate, preferred_element_type=jnp.float32)
    gated_values = (values * jax.nn.sigmoid(gate_pre)).astype(jnp.bfloat16)
    channels = gated_values.shape[1]
    halo_in = jnp.pad(gated_values[tokens - 32 :], ((0, 0), (0, 128 - channels)))

    normed_b = row_norm(expert_in, expert_gain).astype(jnp.bfloat16)
    raised = jnp.exp(route_scores)
    route_weights = raised / jnp.sum(raised, axis=1, keepdims=True)
    served = []
    for j in range(2):
        dz, dx = shift_of(y, c, j)
        served.append(((z + dz) % NZ) * NX + (x + dx) % NX)
    served = jnp.stack(served).astype(jnp.int32)
    hits = route_experts[None, :, :] == served[:, None, None]
    named = jnp.any(hits, axis=2)
    earlier = jnp.arange(tokens)[:, None] < jnp.arange(tokens)[None, :]
    rank = jnp.dot(
        named.astype(jnp.bfloat16), earlier.astype(jnp.bfloat16), preferred_element_type=jnp.float32
    ).astype(jnp.int32)
    chosen = jnp.logical_and(
        named[:, None, :], rank[:, None, :] == jnp.arange(SLOTS, dtype=jnp.int32)[None, :, None]
    ).astype(jnp.bfloat16)
    send = (
        jnp.dot(chosen.reshape(2 * SLOTS, tokens), normed_b, preferred_element_type=jnp.float32)
        .astype(jnp.bfloat16)
        .reshape(2, SLOTS, -1)
    )

    hidden, halo = dispatch(send, halo_in, expert_gate, expert_up)

    first = jnp.logical_and(z == 0, x == 0)
    earlier_rows = jnp.where(first, jnp.zeros_like(halo), halo)[2:, :channels]
    extended = jnp.concatenate([earlier_rows, gated_values], axis=0)
    conv_out = jnp.zeros(gated_values.shape, jnp.float32)
    for offset in range(CONV_W):
        conv_out = (
            conv_out + extended[offset : offset + tokens].astype(jnp.float32) * w_taps[offset]
        )
    stats = jnp.concatenate(
        [
            jnp.sum(conv_out, axis=1)[None],
            jnp.sum(conv_out * conv_out, axis=1)[None],
            jnp.zeros((6, tokens), jnp.float32),
        ]
    )

    returned, stats = combine(hidden, expert_down, stats)

    row_mean = stats[0][:, None] / CONV_CH
    row_var = stats[1][:, None] / CONV_CH - row_mean * row_mean
    activated = jax.nn.silu(
        (conv_out - row_mean) * lax.rsqrt(row_var + epsilon) * channel_gain
    ).astype(jnp.bfloat16)
    part_m = jnp.dot(activated, w_output, preferred_element_type=jnp.float32).astype(jnp.bfloat16)

    weight = jnp.sum(jnp.where(hits, route_weights[None], 0.0), axis=2)
    part_e = jnp.zeros((tokens, returned.shape[2]), jnp.float32)
    for j in range(2):
        picked = lax.dot_general(
            chosen[j], returned[j], (((0,), (0,)), ((), ())), preferred_element_type=jnp.float32
        )
        part_e = part_e + picked * weight[j][:, None]
    return total_over_tp(part_m, part_e.astype(jnp.bfloat16))


def solution(mesh):
    split = Mesh(mesh.devices.reshape(NZ, NX, NY, 2), ("z", "x", "y", "c"))
    in_specs = (
        P(EP, None),
        P(),
        P(None, TP),
        P(None, TP),
        P(None, TP),
        P(TP),
        P(TP, None),
        P(EP, None),
        P(),
        P(EP, None),
        P(EP, None),
        P(EP, None, TP),
        P(EP, None, TP),
        P(EP, TP, None),
    )
    out_specs = (P(EP, None), P(EP, None))
    return jax.shard_map(local, mesh=split, in_specs=in_specs, out_specs=out_specs, check_vma=False)
```

```python
from types import SimpleNamespace

import jax
import jax.numpy as jnp
from jax import lax
from jax.experimental import pallas as pl
from jax.experimental.pallas import tpu as pltpu
from jax.sharding import Mesh
from jax.sharding import PartitionSpec as P

CONV_CH = 1536
CONV_W = 31
EP = ("z", "x")
TP = ("y", "c")
NZ, NX, NY = 8, 4, 8
SLOTS = 32
NEAR = 8
HALF = 1024
FAR = NY // 2

epsilon = 1e-05
clamp_limit = 7.0
swish_slope = 1.702

VM = pl.BlockSpec(memory_space=pltpu.VMEM)
ANY = pl.BlockSpec(memory_space=pl.ANY)
DMA = pltpu.SemaphoreType.DMA


def far_shift(y, c):
    p = y // 4
    dz = (1 - p) * (3 + 2 * c) + p * (4 * (1 - c) + c * (6 - 4 * (y % 2)))
    return dz, y % 4


def near_shift(c, i):
    return (0, 1, NZ - 1, 2 + 4 * c)[i // 2], 2 * (i % 2) + c


def reach(way, j):
    return FAR if way == j else FAR - 1


def put(src, dst, sent, landed, **device):
    return pltpu.make_async_remote_copy(
        src_ref=src,
        dst_ref=dst,
        send_sem=sent,
        recv_sem=landed,
        device_id=device,
        device_id_type=pl.DeviceIdType.MESH,
    )


def place():
    return tuple(lax.axis_index(a) for a in ("z", "x", "y", "c"))


def tiles(count, width, body):
    def step(n, _):
        body(pl.ds(pl.multiple_of(n * width, width), width))
        return 0

    lax.fori_loop(0, count, step, 0)


def mm(a, b):
    return jnp.dot(a, b, preferred_element_type=jnp.float32)


def norm_into(out, inputs, gain):
    def rows(at):
        widened = inputs[at, :].astype(jnp.float32)
        mean = jnp.mean(widened, axis=-1, keepdims=True)
        centred = widened - mean
        var = jnp.mean(jnp.square(centred), axis=-1, keepdims=True)
        out[at, :] = (centred * lax.rsqrt(var + epsilon) * gain[...]).astype(jnp.bfloat16)

    tiles(4, 32, rows)


NAMES = []


def whole_kernel(*refs):
    r = SimpleNamespace(**dict(zip(NAMES, refs)))
    z, x, y, c = place()
    other = 1 - c
    sides = ((y + 1) % NY, (y + NY - 1) % NY)
    block = z * NX + x
    after = (block + 1) % (NZ * NX)
    before = (block + NZ * NX - 1) % (NZ * NX)
    bf16, f32 = jnp.bfloat16, jnp.float32

    def on(dz, dx):
        return dict(z=(z + dz) % NZ, x=(x + dx) % NX)

    def back(dz, dx):
        return dict(z=(z + NZ - dz) % NZ, x=(x + NX - dx) % NX)

    far = far_shift(y, c)
    near = [near_shift(c, i) for i in range(NEAR)]
    itself = c == 0
    not_itself = c == 1

    barrier = pltpu.get_barrier_semaphore()

    def greet(**device):
        pl.semaphore_signal(barrier, inc=1, device_id=device, device_id_type=pl.DeviceIdType.MESH)

    for n, shift in enumerate([far] + near):

        def both(shift=shift):
            greet(**on(*shift))
            greet(**back(*shift))

        if n == 1:
            pl.when(not_itself)(both)
        else:
            both()
    greet(c=other)
    for i in range(1, NY):
        greet(y=(y + i) % NY)
    greet(z=after // NX, x=after % NX)
    greet(z=before // NX, x=before % NX)
    load_sem = r.load_sem

    def load(n, src, dst):
        copy = pltpu.make_async_copy(src, dst, load_sem.at[n])
        copy.start()
        return copy

    load_tokens_b = load(0, r.expert_in, r.tokens_b)
    load_tokens_a = load(1, r.mixer_in, r.tokens_a)
    load_w_value = load(2, r.w_value_in, r.w_value)
    load_w_gate = load(3, r.w_gate_in, r.w_gate)
    load_gate = load(4, r.gate_in.at[0], r.weights.at[:, pl.ds(0, 128)])
    load_up = load(5, r.up_in.at[0], r.weights.at[:, pl.ds(128, 128)])
    load_down = load(6, r.down_in.at[0], r.down)
    load_w_output = load(7, r.w_output_in, r.w_output)

    routes = r.routes[...]
    raised = jnp.exp(r.scores[...])
    route_weights = raised / jnp.sum(raised, axis=0, keepdims=True)
    named, weight = [], []
    for shift in near + [far]:
        target = tuple(on(*shift).values())
        hit = routes == target[0] * NX + target[1]
        named.append(jnp.max(jnp.where(hit, 1.0, 0.0), axis=0, keepdims=True))
        weight.append(jnp.sum(jnp.where(hit, route_weights, 0.0), axis=0, keepdims=True))
    stacked = jnp.concatenate(named + [jnp.zeros((7, 128), f32)], axis=0).astype(bf16)
    sooner = lax.broadcasted_iota(jnp.int32, (128, 128), 0) < lax.broadcasted_iota(
        jnp.int32, (128, 128), 1
    )
    rank = mm(stacked, jnp.where(sooner, 1.0, 0.0).astype(bf16))
    slot = lax.broadcasted_iota(jnp.int32, (SLOTS, 128), 0).astype(f32)
    spread_weights = []
    for n in range(NEAR + 1):
        chosen = jnp.where(rank[n : n + 1] == slot, 1.0, 0.0) * named[n]
        r.pick[n * SLOTS : (n + 1) * SLOTS] = chosen.astype(bf16)
        spread_weights.append(chosen * weight[n])
    spread_weights.append(jnp.zeros((96, 128), f32))
    spread_weights = jnp.concatenate(spread_weights, axis=0)
    for n in range(3):
        turned = spread_weights[n * 128 : (n + 1) * 128].T
        high = turned.astype(bf16)
        r.back_high[n] = high
        r.back_low[n] = (turned - high.astype(f32)).astype(bf16)

    load_tokens_b.wait()
    norm_into(r.normed, r.tokens_b, r.expert_gain)
    normed = r.normed

    def far_columns(at):
        r.far_send[:, at] = mm(r.pick[NEAR * SLOTS :], normed[:, at]).astype(bf16)

    tiles(4, 512, far_columns)
    pl.semaphore_wait(barrier, jnp.where(itself, 26, 28))

    rows_far, rows_near = r.rows_far, r.rows_near

    def half(j):
        return pl.ds(16 * j, 16)

    def far_out(j):
        return put(
            r.far_send.at[half(j)], rows_far.at[y, c, half(j)],
            r.far_sent.at[j], r.far_here.at[j], **on(*far),
        )

    for j in range(2):
        far_out(j).start()

    def near_columns(at):
        r.near_send[:, :, at] = (
            mm(r.pick[: NEAR * SLOTS], normed[:, at]).astype(bf16).reshape(NEAR, SLOTS, 512)
        )

    tiles(4, 512, near_columns)

    def near_out(i):
        return put(
            r.near_send.at[i], rows_near.at[i, c],
            r.near_sent.at[i], r.near_here.at[i], **on(*near[i]),
        )

    stays_out = pltpu.make_async_copy(r.near_send.at[0], rows_near.at[0, c], r.stay_sem.at[0])

    def start_near(make, stay, i):
        if i == 0:
            pl.when(itself)(lambda: stay.start())
            pl.when(not_itself)(lambda: make(0).start())
        else:
            make(i).start()

    def wait_near(make, stay, i):
        if i == 0:
            pl.when(itself)(lambda: stay.wait())
            pl.when(not_itself)(lambda: make(0).wait())
        else:
            make(i).wait()

    for i in range(NEAR):
        start_near(near_out, stays_out, i)

    load_tokens_a.wait()
    norm_into(normed, r.tokens_a, r.mixer_gain)
    load_w_value.wait()
    load_w_gate.wait()
    values = mm(normed[...], r.w_value[...])
    gate_pre = mm(normed[...], r.w_gate[...])
    gated = (values * jax.nn.sigmoid(gate_pre)).astype(bf16)
    extended = r.extended
    extended[32:, :96] = gated.astype(f32)
    r.halo_out[...] = jnp.zeros((32, 128), bf16)
    r.halo_out[:, :96] = gated[96:]
    halo = put(
        r.halo_out, r.halo_in, r.halo_sem.at[0], r.halo_sem.at[1],
        z=after // NX, x=after % NX,
    )
    halo.start()

    def origin(k, way):
        return (y + NY - k) % NY if way == 0 else (y + k) % NY

    def ring(k, j, way):
        piece = rows_far.at[origin(k, way), c, half(j)]
        return put(
            piece, piece, r.ring_sent.at[way, k, j], r.ring_here.at[way, k, j], y=sides[way]
        )

    def relay(k, j, way):
        piece = rows_far.at[origin(k + 1, way), c, half(j)]
        return put(
            piece, piece, r.relay_sent.at[way, k, j], r.relay_here.at[way, k, j], c=other
        )

    def own(j):
        piece = rows_far.at[y, c, half(j)]
        return put(piece, piece, r.own_sent.at[j], r.own_here.at[j], c=other)

    def near_relay(i):
        piece = rows_near.at[i, c]
        return put(piece, piece, r.nrelay_sent.at[i], r.nrelay_here.at[i], c=other)

    def product(hidden, rows, at):
        both = mm(rows[at].reshape(2 * SLOTS, 2048), r.weights[...])
        gate = jnp.minimum(both[:, :128], clamp_limit)
        up = jnp.clip(both[:, 128:], -clamp_limit, clamp_limit)
        hidden[at] = (
            ((up + 1.0) * gate * jax.nn.sigmoid(swish_slope * gate))
            .astype(bf16)
            .reshape(2, SLOTS, 128)
        )

    hidden_far, hidden_near = r.hidden_far, r.hidden_near

    def near_in(i):
        wait_near(near_out, stays_out, i)
        near_relay(i).start()

    def near_product(i):
        near_relay(i).wait()
        product(hidden_near, rows_near, i)

    for j in range(2):
        far_out(j).wait()
        for way in range(2):
            ring(0, j, way).start()
        own(j).start()

    halo.wait()
    keep = jnp.where(block == 0, 0.0, 1.0)
    extended[:32, :96] = r.halo_in[:, :96].astype(f32) * keep
    conv = jnp.zeros((128, 96), f32)
    for tap in range(CONV_W):
        conv = conv + extended[2 + tap : 130 + tap, :96] * r.w_taps[tap : tap + 1, :]
    r.conv[...] = conv
    lane = lax.broadcasted_iota(jnp.int32, (128, 128), 1)
    sums = jnp.sum(conv, axis=1, keepdims=True)
    squares = jnp.sum(conv * conv, axis=1, keepdims=True)
    columns = jnp.where(lane == 0, sums, jnp.where(lane == 1, squares, 0.0))
    r.stats[...] = columns.T[:8]

    def stats_swap():
        return put(r.stats, r.stats_pair, r.swap_sem.at[0], r.swap_sem.at[1], c=other)

    def stats_spread(i):
        return put(
            r.stats_sum, r.stats_all.at[y], r.stats_sent.at[i], r.stats_here.at[i],
            y=(y + i) % NY,
        )

    stats_swap().start()
    load_gate.wait()
    load_up.wait()

    for k in range(FAR):
        for j in range(2):
            for way in range(2):
                if k < reach(way, j):
                    ring(k, j, way).wait_recv()
                    if k + 1 < reach(way, j):
                        ring(k + 1, j, way).start()
                    relay(k, j, way).start()
        if k == 0:
            own(0).wait()
            own(1).wait()
            product(hidden_far, rows_far, y)
            stats_swap().wait()
            r.stats_sum[...] = r.stats[...] + r.stats_pair[...]
            for i in range(1, NY):
                stats_spread(i).start()
        else:
            near_product(2 * k - 2)
            near_product(2 * k - 1)
        near_in(2 * k)
        near_in(2 * k + 1)
        for j in range(2):
            for way in range(2):
                if k < reach(way, j):
                    relay(k, j, way).wait_recv()
        for way in range(2 if k < FAR - 1 else 1):
            product(hidden_far, rows_far, origin(k + 1, way))

    def away(m, way):
        return (y + m) % NY if way == 0 else (y + NY - m) % NY

    order = [(FAR, 0)] + [(m, way) for m in range(FAR - 1, 0, -1) for way in range(2)] + [(0, 0)]
    mine, given, taken = r.mine, r.given, r.taken
    chain_in, chain_out = r.chain_in, r.chain_out
    load_down.wait()

    def gift(i):
        return put(given.at[i], taken.at[i], r.gift_sent.at[i], r.gift_here.at[i], c=other)

    def partial(i):
        dest = away(*order[i])

        def cols(at):
            mine[i, :, at] = mm(hidden_far[dest, c], r.down[:, at])
            given[i, :, at] = mm(hidden_far[dest, other], r.down[:, at]).astype(bf16)

        tiles(4, 512, cols)
        gift(i).start()

    def settle(i):
        gift(i).wait_recv()

    def chain(m, j, way):
        return put(
            chain_out.at[way, m - 1, j], chain_in.at[way, m - 1, j],
            r.chain_sent.at[way, m - 1, j], r.chain_here.at[way, m - 1, j], y=sides[way],
        )

    def so_far(i, j):
        return mine[i, 16 * j : 16 * j + 16] + taken[i, 16 * j : 16 * j + 16].astype(f32)

    def pass_on(m, j, way, i):
        total = so_far(i, j)
        if m < reach(way, j):
            chain(m + 1, j, way).wait_recv()
            total = total + chain_in[way, m, j].astype(f32)
        chain_out[way, m - 1, j] = total.astype(bf16)
        chain(m, j, way).start()

    def near_gift(b):
        at = pl.ds(4 * b, 4)
        return put(
            r.near_given.at[at], r.near_taken.at[at],
            r.ngift_sent.at[b], r.ngift_here.at[b], c=other,
        )

    def near_give():
        def cols(at):
            r.near_given[:, :, at] = (
                mm(hidden_near[:, other].reshape(NEAR * SLOTS, 128), r.down[:, at])
                .astype(bf16)
                .reshape(NEAR, SLOTS, 512)
            )

        tiles(4, 512, cols)
        near_gift(0).start()
        near_gift(1).start()

    def near_back(i):
        return put(
            r.near_ready.at[i], r.near_got.at[i],
            r.nback_sent.at[i], r.nback_here.at[i], **back(*near[i]),
        )

    stays_back = pltpu.make_async_copy(
        r.near_ready.at[0], r.near_got.at[0], r.stay_sem.at[1]
    )

    def near_return(b):
        near_gift(b).wait_recv()
        blocks = pl.ds(4 * b, 4)

        def cols(at):
            done = mm(hidden_near[blocks, c].reshape(4 * SLOTS, 128), r.down[:, at])
            r.near_ready[blocks, :, at] = (
                done.reshape(4, SLOTS, 512) + r.near_taken[blocks, :, at].astype(f32)
            ).astype(bf16)

        tiles(4, 512, cols)
        for i in range(4 * b, 4 * b + 4):
            start_near(near_back, stays_back, i)

    mine_at = pl.ds(pl.multiple_of(c * HALF, HALF), HALF)
    their_at = pl.ds(pl.multiple_of(other * HALF, HALF), HALF)
    outs = (r.out_m, r.out_e)
    rounds = (4, 3, 5, 2, 6, 1, 7)

    def part_gift(o):
        return put(
            r.part.at[o, :, :, their_at], r.part_taken.at[o],
            r.pgift_sent.at[o], r.pgift_here.at[o], c=other,
        )

    def scatter(o, i):
        return put(
            r.halves.at[o, (y + i) % NY], r.arrived.at[o, y],
            r.scat_sent.at[o, i], r.scat_here.at[o, i], y=(y + i) % NY,
        )

    def scatter_all(o):
        part_gift(o).wait_recv()
        r.halves[o] = (
            r.part[o, :, :, mine_at].astype(f32) + r.part_taken[o].astype(f32)
        ).astype(bf16)
        for i in rounds:
            scatter(o, i).start()

    def publish(o, i):
        piece = outs[o].at[y, :, mine_at]
        return put(
            piece, piece, r.pub_sent.at[o, i], r.pub_here.at[o, i], y=(y + i) % NY
        )

    def share(o, i):
        piece = outs[o].at[(y + NY - i) % NY, :, mine_at]
        return put(piece, piece, r.share_sent.at[o, i], r.share_here.at[o, i], c=other)

    def publish_all(o):
        total = r.part[o, y, :, mine_at].astype(f32) + r.part_taken[o, y].astype(f32)
        for i in reversed(rounds):
            scatter(o, i).wait_recv()
            total = total + r.arrived[o, (y + NY - i) % NY].astype(f32)
        outs[o][y, :, mine_at] = total.astype(bf16)
        for i in rounds:
            publish(o, i).start()
        share(o, 0).start()

    def share_all(o):
        for i in reversed(rounds):
            publish(o, i).wait_recv()
            share(o, i).start()

    def mixer_part():
        total = r.stats_sum[...]
        for i in range(1, NY):
            stats_spread(i).wait()
            total = total + r.stats_all[(y + NY - i) % NY]
        turned = jnp.concatenate([total, jnp.zeros((120, 128), f32)], axis=0).T
        row_mean = turned[:, 0:1] / CONV_CH
        row_var = turned[:, 1:2] / CONV_CH - row_mean * row_mean
        scaled = (r.conv[...] - row_mean) * lax.rsqrt(row_var + epsilon)
        scaled = scaled * r.channel_gain[...]
        activated = (scaled * jax.nn.sigmoid(scaled)).astype(bf16)
        load_w_output.wait()

        def cols(at):
            r.part[0, :, :, at] = (
                mm(activated, r.w_output[:, at]).astype(bf16).reshape(NY, 16, 512)
            )

        tiles(4, 512, cols)
        part_gift(0).start()

    partial(0)
    partial(1)
    partial(2)
    settle(0)
    pass_on(FAR, 0, 0, 0)
    pass_on(FAR, 1, 1, 0)
    for m in range(FAR - 1, 0, -1):
        i = 1 + 2 * (FAR - 1 - m)
        partial(i + 2)
        if m > 1:
            partial(i + 3)
        if m == 3:
            near_product(6)
            near_product(7)
        settle(i)
        settle(i + 1)
        for turn in range(2):
            for way in range(2):
                pass_on(m, 1 - way if turn == 0 else way, way, i + way)
        if m == 3:
            near_give()
            mixer_part()
        elif m == 2:
            near_return(0)
            scatter_all(0)
        else:
            near_return(1)
    last = len(order) - 1
    settle(last)

    def far_back(j):
        return put(
            r.far_ready.at[half(j)], r.far_got.at[half(j)],
            r.fback_sent.at[j], r.fback_here.at[j], **back(*far),
        )

    for j in range(2):
        chain(1, j, 0).wait_recv()
        chain(1, j, 1).wait_recv()
        r.far_ready[16 * j : 16 * j + 16] = (
            so_far(last, j) + chain_in[0, 0, j].astype(f32) + chain_in[1, 0, j].astype(f32)
        ).astype(bf16)
        far_back(j).start()

    publish_all(0)
    for i in range(NEAR):
        wait_near(near_back, stays_back, i)

    def near_sum(at):
        total = jnp.zeros((128, 512), f32)
        for n in range(2):
            got = r.near_got[4 * n : 4 * n + 4, :, at].reshape(128, 512)
            total = total + mm(r.back_high[n], got) + mm(r.back_low[n], got)
        r.summed[:, at] = total

    tiles(4, 512, near_sum)
    share_all(0)
    for j in range(2):
        far_back(j).wait()

    def far_sum(at):
        got = r.far_got[:, at]
        total = (
            r.summed[:, at]
            + mm(r.back_high[2, :, :SLOTS], got)
            + mm(r.back_low[2, :, :SLOTS], got)
        )
        r.part[1, :, :, at] = total.astype(bf16).reshape(NY, 16, 512)

    tiles(4, 512, far_sum)
    part_gift(1).start()
    scatter_all(1)
    publish_all(1)
    share_all(1)

    for j in range(2):
        for way in range(2):
            for k in range(reach(way, j)):
                ring(k, j, way).wait_send()
                relay(k, j, way).wait_send()
                chain(k + 1, j, way).wait_send()
    for i in range(len(order)):
        gift(i).wait_send()
    near_gift(0).wait_send()
    near_gift(1).wait_send()
    for o in range(2):
        part_gift(o).wait_send()
        share(o, 0).wait()
        for i in rounds:
            scatter(o, i).wait_send()
            publish(o, i).wait_send()
            share(o, i).wait()


def vm(*shape, dtype=jnp.bfloat16):
    return pltpu.VMEM(shape, dtype)


INPUTS = dict(
    mixer_in=ANY, mixer_gain=VM, w_value_in=ANY, w_gate_in=ANY, w_taps=VM,
    channel_gain=VM, w_output_in=ANY, expert_in=ANY, expert_gain=VM, routes=VM,
    scores=VM, gate_in=ANY, up_in=ANY, down_in=ANY,
)
F32 = jnp.float32
SCRATCH = dict(
    tokens_b=vm(128, 2048), tokens_a=vm(128, 2048), normed=vm(128, 2048),
    w_value=vm(2048, 96), w_gate=vm(2048, 96), weights=vm(2048, 256),
    down=vm(128, 2048), w_output=vm(96, 2048), pick=vm((NEAR + 1) * SLOTS, 128),
    back_high=vm(3, 128, 128), back_low=vm(3, 128, 128),
    far_send=vm(SLOTS, 2048), near_send=vm(NEAR, SLOTS, 2048),
    rows_far=vm(NY, 2, SLOTS, 2048), rows_near=vm(NEAR, 2, SLOTS, 2048),
    hidden_far=vm(NY, 2, SLOTS, 128), hidden_near=vm(NEAR, 2, SLOTS, 128),
    extended=vm(160, 128, dtype=F32), halo_out=vm(32, 128), halo_in=vm(32, 128),
    conv=vm(128, 96, dtype=F32), stats=vm(8, 128, dtype=F32),
    stats_pair=vm(8, 128, dtype=F32), stats_sum=vm(8, 128, dtype=F32),
    stats_all=vm(NY, 8, 128, dtype=F32), mine=vm(NY, SLOTS, 2048, dtype=F32),
    given=vm(NY, SLOTS, 2048), taken=vm(NY, SLOTS, 2048),
    chain_in=vm(2, FAR, 2, 16, 2048), chain_out=vm(2, FAR, 2, 16, 2048),
    near_given=vm(NEAR, SLOTS, 2048), near_taken=vm(NEAR, SLOTS, 2048),
    near_ready=vm(NEAR, SLOTS, 2048), near_got=vm(NEAR, SLOTS, 2048),
    far_ready=vm(SLOTS, 2048), far_got=vm(SLOTS, 2048), summed=vm(128, 2048, dtype=F32),
    part=vm(2, NY, 16, 2048), part_taken=vm(2, NY, 16, HALF), halves=vm(2, NY, 16, HALF),
    arrived=vm(2, NY, 16, HALF),
    load_sem=DMA((8,)), far_sent=DMA((2,)), far_here=DMA((2,)),
    near_sent=DMA((NEAR,)), near_here=DMA((NEAR,)), stay_sem=DMA((2,)),
    halo_sem=DMA((2,)), ring_sent=DMA((2, FAR, 2)), ring_here=DMA((2, FAR, 2)),
    relay_sent=DMA((2, FAR, 2)), relay_here=DMA((2, FAR, 2)), own_sent=DMA((2,)),
    own_here=DMA((2,)), nrelay_sent=DMA((NEAR,)), nrelay_here=DMA((NEAR,)),
    swap_sem=DMA((2,)), stats_sent=DMA((NY,)), stats_here=DMA((NY,)),
    gift_sent=DMA((NY,)), gift_here=DMA((NY,)), chain_sent=DMA((2, FAR, 2)),
    chain_here=DMA((2, FAR, 2)), ngift_sent=DMA((2,)), ngift_here=DMA((2,)),
    nback_sent=DMA((NEAR,)), nback_here=DMA((NEAR,)), fback_sent=DMA((2,)),
    fback_here=DMA((2,)), pgift_sent=DMA((2,)), pgift_here=DMA((2,)),
    scat_sent=DMA((2, NY)), scat_here=DMA((2, NY)), pub_sent=DMA((2, NY)),
    pub_here=DMA((2, NY)), share_sent=DMA((2, NY)), share_here=DMA((2, NY)),
)
NAMES += list(INPUTS | dict(out_m=VM, out_e=VM) | SCRATCH)


def local(
    mixer_in,
    mixer_gain,
    w_value,
    w_gate,
    w_taps,
    channel_gain,
    w_output,
    expert_in,
    expert_gain,
    route_experts,
    route_scores,
    expert_gate,
    expert_up,
    expert_down,
):
    shape = (NY, 16, 2048)
    out_m, out_e = pl.pallas_call(
        whole_kernel,
        out_shape=(jax.ShapeDtypeStruct(shape, jnp.bfloat16),) * 2,
        in_specs=list(INPUTS.values()),
        out_specs=(VM, VM),
        scratch_shapes=list(SCRATCH.values()),
        compiler_params=pltpu.CompilerParams(
            collective_id=0, has_side_effects=True, vmem_limit_bytes=48 << 20
        ),
        name="whole",
    )(
        mixer_in, mixer_gain[None], w_value, w_gate, w_taps, channel_gain[None], w_output,
        expert_in, expert_gain[None], route_experts.T, route_scores.T,
        expert_gate, expert_up, expert_down,
    )
    return out_m.reshape(-1, 2048), out_e.reshape(-1, 2048)


def solution(mesh):
    split = Mesh(mesh.devices.reshape(NZ, NX, NY, 2), ("z", "x", "y", "c"))
    in_specs = (
        P(EP, None),
        P(),
        P(None, TP),
        P(None, TP),
        P(None, TP),
        P(TP),
        P(TP, None),
        P(EP, None),
        P(),
        P(EP, None),
        P(EP, None),
        P(EP, None, TP),
        P(EP, None, TP),
        P(EP, TP, None),
    )
    out_specs = (P(EP, None), P(EP, None))
    return jax.shard_map(local, mesh=split, in_specs=in_specs, out_specs=out_specs, check_vma=False)
```

```python
from types import SimpleNamespace

import jax
import jax.numpy as jnp
from jax import lax
from jax.experimental import pallas as pl
from jax.experimental.pallas import tpu as pltpu
from jax.sharding import Mesh
from jax.sharding import PartitionSpec as P

CONV_CH = 1536
CONV_W = 31
EP = ("z", "x")
TP = ("y", "c")
NZ, NX, NY = 8, 4, 8
SLOTS = 32
NEAR = 8
HALF = 1024
FAR = NY // 2

epsilon = 1e-05
clamp_limit = 7.0
swish_slope = 1.702

VM = pl.BlockSpec(memory_space=pltpu.VMEM)
ANY = pl.BlockSpec(memory_space=pl.ANY)
DMA = pltpu.SemaphoreType.DMA


def far_shift(y, c):
    p = y // 4
    dz = (1 - p) * (3 + 2 * c) + p * (4 * (1 - c) + c * (6 - 4 * (y % 2)))
    return dz, y % 4


def near_shift(c, i):
    return (0, 1, NZ - 1, 2 + 4 * c)[i // 2], 2 * (i % 2) + c


def reach(way, j):
    return FAR if way == j else FAR - 1


def put(src, dst, sent, landed, **device):
    return pltpu.make_async_remote_copy(
        src_ref=src,
        dst_ref=dst,
        send_sem=sent,
        recv_sem=landed,
        device_id=device,
        device_id_type=pl.DeviceIdType.MESH,
    )


def place():
    return tuple(lax.axis_index(a) for a in ("z", "x", "y", "c"))


def tiles(count, width, body):
    def step(n, _):
        body(pl.ds(pl.multiple_of(n * width, width), width))
        return 0

    lax.fori_loop(0, count, step, 0)


def mm(a, b):
    return jnp.dot(a, b, preferred_element_type=jnp.float32)


def norm_into(out, inputs, gain):
    def rows(at):
        widened = inputs[at, :].astype(jnp.float32)
        mean = jnp.mean(widened, axis=-1, keepdims=True)
        centred = widened - mean
        var = jnp.mean(jnp.square(centred), axis=-1, keepdims=True)
        out[at, :] = (centred * lax.rsqrt(var + epsilon) * gain[...]).astype(jnp.bfloat16)

    tiles(4, 32, rows)


NAMES = []


def whole_kernel(*refs):
    r = SimpleNamespace(**dict(zip(NAMES, refs)))
    z, x, y, c = place()
    other = 1 - c
    sides = ((y + 1) % NY, (y + NY - 1) % NY)
    block = z * NX + x
    after = (block + 1) % (NZ * NX)
    before = (block + NZ * NX - 1) % (NZ * NX)
    bf16, f32 = jnp.bfloat16, jnp.float32

    def on(dz, dx):
        return dict(z=(z + dz) % NZ, x=(x + dx) % NX)

    def back(dz, dx):
        return dict(z=(z + NZ - dz) % NZ, x=(x + NX - dx) % NX)

    far = far_shift(y, c)
    near = [near_shift(c, i) for i in range(NEAR)]
    itself = c == 0
    not_itself = c == 1

    barrier = pltpu.get_barrier_semaphore()

    def greet(**device):
        pl.semaphore_signal(barrier, inc=1, device_id=device, device_id_type=pl.DeviceIdType.MESH)

    for n, shift in enumerate([far] + near):

        def both(shift=shift):
            greet(**on(*shift))
            greet(**back(*shift))

        if n == 1:
            pl.when(not_itself)(both)
        else:
            both()
    greet(c=other)
    for i in range(1, NY):
        greet(y=(y + i) % NY)
    greet(z=after // NX, x=after % NX)
    greet(z=before // NX, x=before % NX)
    load_sem = r.load_sem

    def load(n, src, dst):
        copy = pltpu.make_async_copy(src, dst, load_sem.at[n])
        copy.start()
        return copy

    load_tokens_b = load(0, r.expert_in, r.tokens_b)
    load_tokens_a = load(1, r.mixer_in, r.tokens_a)
    load_w_value = load(2, r.w_value_in, r.w_value)
    load_w_gate = load(3, r.w_gate_in, r.w_gate)
    load_gate = load(4, r.gate_in.at[0], r.weights.at[:, pl.ds(0, 128)])
    load_up = load(5, r.up_in.at[0], r.weights.at[:, pl.ds(128, 128)])
    load_down = load(6, r.down_in.at[0], r.down)
    load_w_output = load(7, r.w_output_in, r.w_output)

    routes = r.routes[...]
    raised = jnp.exp(r.scores[...])
    route_weights = raised / jnp.sum(raised, axis=0, keepdims=True)
    named, weight = [], []
    for shift in near + [far]:
        target = tuple(on(*shift).values())
        hit = routes == target[0] * NX + target[1]
        named.append(jnp.max(jnp.where(hit, 1.0, 0.0), axis=0, keepdims=True))
        weight.append(jnp.sum(jnp.where(hit, route_weights, 0.0), axis=0, keepdims=True))
    stacked = jnp.concatenate(named + [jnp.zeros((7, 128), f32)], axis=0).astype(bf16)
    sooner = lax.broadcasted_iota(jnp.int32, (128, 128), 0) < lax.broadcasted_iota(
        jnp.int32, (128, 128), 1
    )
    rank = mm(stacked, jnp.where(sooner, 1.0, 0.0).astype(bf16))
    slot = lax.broadcasted_iota(jnp.int32, (SLOTS, 128), 0).astype(f32)
    spread_weights = []
    for n in range(NEAR + 1):
        chosen = jnp.where(rank[n : n + 1] == slot, 1.0, 0.0) * named[n]
        r.pick[n * SLOTS : (n + 1) * SLOTS] = chosen.astype(bf16)
        spread_weights.append(chosen * weight[n])
    spread_weights.append(jnp.zeros((96, 128), f32))
    spread_weights = jnp.concatenate(spread_weights, axis=0)
    for n in range(3):
        turned = spread_weights[n * 128 : (n + 1) * 128].T
        high = turned.astype(bf16)
        r.back_high[n] = high
        r.back_low[n] = (turned - high.astype(f32)).astype(bf16)

    load_tokens_b.wait()
    norm_into(r.normed, r.tokens_b, r.expert_gain)
    normed = r.normed

    def far_columns(at):
        r.far_send[:, at] = mm(r.pick[NEAR * SLOTS :], normed[:, at]).astype(bf16)

    tiles(4, 512, far_columns)
    pl.semaphore_wait(barrier, jnp.where(itself, 26, 28))

    rows_far, rows_near = r.rows_far, r.rows_near

    def half(j):
        return pl.ds(16 * j, 16)

    def far_out(j):
        return put(
            r.far_send.at[half(j)], rows_far.at[y, c, half(j)],
            r.far_sent.at[j], r.far_here.at[j], **on(*far),
        )

    for j in range(2):
        far_out(j).start()

    load_tokens_a.wait()
    norm_into(r.normed_a, r.tokens_a, r.mixer_gain)
    load_w_value.wait()
    load_w_gate.wait()

    def project(w):
        return lax.dot_general(
            r.normed_a[...], w[...], (((1,), (1,)), ((), ())), preferred_element_type=f32
        )

    values = project(r.w_value)
    gate_pre = project(r.w_gate)
    gated = (values * jax.nn.sigmoid(gate_pre)).astype(bf16)
    extended = r.extended
    extended[32:, :96] = gated.astype(f32)
    r.halo_out[...] = jnp.zeros((32, 128), bf16)
    r.halo_out[:, :96] = gated[96:]
    halo = put(
        r.halo_out, r.halo_in, r.halo_sem.at[0], r.halo_sem.at[1],
        z=after // NX, x=after % NX,
    )
    halo.start()

    def near_columns(at):
        r.near_send[:, :, at] = (
            mm(r.pick[: NEAR * SLOTS], normed[:, at]).astype(bf16).reshape(NEAR, SLOTS, 512)
        )

    tiles(4, 512, near_columns)

    def near_out(i):
        return put(
            r.near_send.at[i], rows_near.at[i, c],
            r.near_sent.at[i], r.near_here.at[i], **on(*near[i]),
        )

    stays_out = pltpu.make_async_copy(r.near_send.at[0], rows_near.at[0, c], r.stay_sem.at[0])

    def start_near(make, stay, i):
        if i == 0:
            pl.when(itself)(lambda: stay.start())
            pl.when(not_itself)(lambda: make(0).start())
        else:
            make(i).start()

    def wait_near(make, stay, i):
        if i == 0:
            pl.when(itself)(lambda: stay.wait())
            pl.when(not_itself)(lambda: make(0).wait())
        else:
            make(i).wait()

    for i in range(NEAR):
        start_near(near_out, stays_out, i)

    def origin(k, way):
        return (y + NY - k) % NY if way == 0 else (y + k) % NY

    def ring(k, j, way):
        piece = rows_far.at[origin(k, way), c, half(j)]
        return put(
            piece, piece, r.ring_sent.at[way, k, j], r.ring_here.at[way, k, j], y=sides[way]
        )

    def relay(k, j, way):
        piece = rows_far.at[origin(k + 1, way), c, half(j)]
        return put(
            piece, piece, r.relay_sent.at[way, k, j], r.relay_here.at[way, k, j], c=other
        )

    def own(j):
        piece = rows_far.at[y, c, half(j)]
        return put(piece, piece, r.own_sent.at[j], r.own_here.at[j], c=other)

    def near_relay(i):
        piece = rows_near.at[i, c]
        return put(piece, piece, r.nrelay_sent.at[i], r.nrelay_here.at[i], c=other)

    hidden_far, hidden_near = r.hidden_far, r.hidden_near

    def product(inputs):
        both = mm(inputs, r.weights[...])
        gate = jnp.minimum(both[:, :128], clamp_limit)
        up = jnp.clip(both[:, 128:], -clamp_limit, clamp_limit)
        return ((up + 1.0) * gate * jax.nn.sigmoid(swish_slope * gate)).astype(bf16)

    def far_product(sources):
        inputs = [rows_far[source].reshape(2 * SLOTS, 2048) for source in sources]
        outputs = product(jnp.concatenate(inputs, axis=0) if len(inputs) > 1 else inputs[0])
        for n, source in enumerate(sources):
            hidden_far[source] = outputs[n * 64 : n * 64 + 64].reshape(2, SLOTS, 128)

    def near_in(i):
        wait_near(near_out, stays_out, i)
        near_relay(i).start()

    def near_product(b):
        for i in range(4 * b, 4 * b + 4):
            near_relay(i).wait()
        at = pl.ds(4 * b, 4)
        hidden_near[at] = product(rows_near[at].reshape(8 * SLOTS, 2048)).reshape(4, 2, SLOTS, 128)

    def away(m, way):
        return (y + m) % NY if way == 0 else (y + NY - m) % NY

    mine, given, taken = r.mine, r.given, r.taken
    chain_in, chain_out = r.chain_in, r.chain_out

    def first_of(m):
        return 0 if m == FAR else 1 + 2 * (FAR - 1 - m)

    def gift(m):
        at = pl.ds(first_of(m), 1 if m in (0, FAR) else 2)
        return put(given.at[at], taken.at[at], r.gift_sent.at[m], r.gift_here.at[m], c=other)

    def partial(m):
        dests = [away(m, way) for way in range(1 if m in (0, FAR) else 2)]
        inputs = [hidden_far[dest, core] for core in (c, other) for dest in dests]
        inputs = jnp.concatenate(inputs, axis=0)
        count = len(dests)
        at_m = pl.ds(first_of(m), count)

        def cols(at):
            done = mm(inputs, r.down[:, at]).reshape(2, count, SLOTS, 512)
            mine[at_m, :, at] = done[0]
            given[at_m, :, at] = done[1].astype(bf16)

        tiles(4, 512, cols)
        gift(m).start()

    def chain(m, j, way):
        return put(
            chain_out.at[way, m - 1, j], chain_in.at[way, m - 1, j],
            r.chain_sent.at[way, m - 1, j], r.chain_here.at[way, m - 1, j], y=sides[way],
        )

    def so_far(i, j):
        return mine[i, 16 * j : 16 * j + 16] + taken[i, 16 * j : 16 * j + 16].astype(f32)

    def pass_on(m, j, way):
        total = so_far(first_of(m) + (0 if m == FAR else way), j)
        if m < reach(way, j):
            chain(m + 1, j, way).wait_recv()
            total = total + chain_in[way, m, j].astype(f32)
        chain_out[way, m - 1, j] = total.astype(bf16)
        chain(m, j, way).start()

    def near_gift(b):
        at = pl.ds(4 * b, 4)
        return put(
            r.near_given.at[at], r.near_taken.at[at], r.ngift_sent.at[b], r.ngift_here.at[b], c=other
        )

    def near_give(b):
        blocks = pl.ds(4 * b, 4)
        inputs = hidden_near[blocks, other].reshape(4 * SLOTS, 128)

        def cols(at):
            done = mm(inputs, r.down[:, at]).astype(bf16)
            r.near_given[blocks, :, at] = done.reshape(4, SLOTS, 512)

        tiles(4, 512, cols)
        near_gift(b).start()

    def near_back(i):
        return put(
            r.near_ready.at[i], r.near_got.at[i],
            r.nback_sent.at[i], r.nback_here.at[i], **back(*near[i]),
        )

    stays_back = pltpu.make_async_copy(r.near_ready.at[0], r.near_got.at[0], r.stay_sem.at[1])

    def near_return(b):
        near_gift(b).wait_recv()
        blocks = pl.ds(4 * b, 4)
        inputs = hidden_near[blocks, c].reshape(4 * SLOTS, 128)

        def cols(at):
            done = mm(inputs, r.down[:, at])
            r.near_ready[blocks, :, at] = (
                done.reshape(4, SLOTS, 512) + r.near_taken[blocks, :, at].astype(f32)
            ).astype(bf16)

        tiles(4, 512, cols)
        for i in range(4 * b, 4 * b + 4):
            start_near(near_back, stays_back, i)

    mine_at = pl.ds(pl.multiple_of(c * HALF, HALF), HALF)
    their_at = pl.ds(pl.multiple_of(other * HALF, HALF), HALF)
    outs = (r.out_m, r.out_e)
    rounds = (4, 3, 5, 2, 6, 1, 7)

    def part_gift(o):
        return put(
            r.part.at[o, :, :, their_at], r.part_taken.at[o],
            r.pgift_sent.at[o], r.pgift_here.at[o], c=other,
        )

    def scatter(i):
        return put(
            r.halves.at[1, (y + i) % NY], r.arrived.at[y],
            r.scat_sent.at[i], r.scat_here.at[i], y=(y + i) % NY,
        )

    def scatter_all():
        part_gift(1).wait_recv()
        r.halves[1] = (
            r.part[1, :, :, mine_at].astype(f32) + r.part_taken[1].astype(f32)
        ).astype(bf16)
        for i in rounds:
            scatter(i).start()

    def publish(o, i):
        piece = outs[o].at[y, :, mine_at]
        return put(
            piece, piece, r.pub_sent.at[o, i], r.pub_here.at[o, i], y=(y + i) % NY
        )

    def share(o, i):
        piece = outs[o].at[(y + NY - i) % NY, :, mine_at]
        return put(piece, piece, r.share_sent.at[o, i], r.share_here.at[o, i], c=other)

    def publish_all():
        total = r.part[1, y, :, mine_at].astype(f32) + r.part_taken[1, y].astype(f32)
        for i in reversed(rounds):
            scatter(i).wait_recv()
            total = total + r.arrived[(y + NY - i) % NY].astype(f32)
        outs[1][y, :, mine_at] = total.astype(bf16)
        for i in rounds:
            publish(1, i).start()
        share(1, 0).start()

    def share_all(o):
        for i in reversed(rounds):
            publish(o, i).wait_recv()
            share(o, i).start()

    def mixer_part():
        total = r.stats_sum[...]
        for i in range(1, NY):
            stats_spread(i).wait()
            total = total + r.stats_all[(y + NY - i) % NY]
        turned = jnp.concatenate([total, jnp.zeros((120, 128), f32)], axis=0).T
        row_mean = turned[:, 0:1] / CONV_CH
        row_var = turned[:, 1:2] / CONV_CH - row_mean * row_mean
        scaled = (r.conv[...] - row_mean) * lax.rsqrt(row_var + epsilon)
        scaled = scaled * r.channel_gain[...]
        activated = (scaled * jax.nn.sigmoid(scaled)).astype(bf16)
        load_w_output.wait()

        def cols(at):
            r.part[0, :, :, at] = (
                mm(activated, r.w_output[:, at]).astype(bf16).reshape(NY, 16, 512)
            )

        tiles(4, 512, cols)
        part_gift(0).start()

    def mixer_own(dest, j):
        at = slice(512 * j, 512 * j + 512)
        return r.halves[0, dest, :, at].astype(f32)

    def mixer_chain(m, j, way):
        return put(
            r.mchain_out.at[way, m - 1, j], r.mchain_in.at[way, m - 1, j],
            r.mchain_sent.at[way, m - 1, j], r.mchain_here.at[way, m - 1, j], y=sides[way],
        )

    def mixer_pass(m, j, way):
        total = mixer_own(away(m, way), j)
        if m < reach(way, j):
            mixer_chain(m + 1, j, way).wait_recv()
            total = total + r.mchain_in[way, m, j].astype(f32)
        r.mchain_out[way, m - 1, j] = total.astype(bf16)
        mixer_chain(m, j, way).start()

    def mixer_publish():
        for j in range(2):
            total = mixer_own(y, j)
            for way in range(2):
                mixer_chain(1, j, way).wait_recv()
                total = total + r.mchain_in[way, 0, j].astype(f32)
            r.out_m[y, :, pl.ds(pl.multiple_of(c * HALF + 512 * j, 512), 512)] = total.astype(bf16)
        for i in rounds:
            publish(0, i).start()
        share(0, 0).start()

    def conv_and_stats():
        halo.wait()
        keep = jnp.where(block == 0, 0.0, 1.0)
        extended[:32, :96] = r.halo_in[:, :96].astype(f32) * keep
        conv = jnp.zeros((128, 96), f32)
        for tap in range(CONV_W):
            conv = conv + extended[2 + tap : 130 + tap, :96] * r.w_taps[tap : tap + 1, :]
        r.conv[...] = conv
        lane = lax.broadcasted_iota(jnp.int32, (128, 128), 1)
        sums = jnp.sum(conv, axis=1, keepdims=True)
        squares = jnp.sum(conv * conv, axis=1, keepdims=True)
        columns = jnp.where(lane == 0, sums, jnp.where(lane == 1, squares, 0.0))
        r.stats[...] = columns.T[:8]
        stats_swap().start()

    def stats_spread(i):
        return put(
            r.stats_sum, r.stats_all.at[y], r.stats_sent.at[i], r.stats_here.at[i],
            y=(y + i) % NY,
        )

    def stats_swap():
        return put(r.stats, r.stats_pair, r.swap_sem.at[0], r.swap_sem.at[1], c=other)

    load_gate.wait()
    load_up.wait()
    load_down.wait()
    for j in range(2):
        far_out(j).wait()
        for way in range(2):
            ring(0, j, way).start()
        own(j).start()
    conv_and_stats()
    own(0).wait()
    own(1).wait()
    far_product([y])
    partial(0)
    for k in range(FAR):
        for j in range(2):
            for way in range(2):
                if k < reach(way, j):
                    ring(k, j, way).wait_recv()
                    if k + 1 < reach(way, j):
                        ring(k + 1, j, way).start()
                    relay(k, j, way).start()
        near_in(2 * k)
        near_in(2 * k + 1)
        if k == 0:
            stats_swap().wait()
            r.stats_sum[...] = r.stats[...] + r.stats_pair[...]
            for i in range(1, NY):
                stats_spread(i).start()
        elif k == 2:
            near_product(0)
        elif k == 3:
            mixer_part()
        for j in range(2):
            for way in range(2):
                if k < reach(way, j):
                    relay(k, j, way).wait_recv()
        far_product([origin(k + 1, way) for way in range(2 if k < FAR - 1 else 1)])
        partial(k + 1)

    gift(FAR).wait_recv()
    pass_on(FAR, 0, 0)
    pass_on(FAR, 1, 1)
    part_gift(0).wait_recv()
    r.halves[0] = (
        r.part[0, :, :, mine_at].astype(f32) + r.part_taken[0].astype(f32)
    ).astype(bf16)
    mixer_pass(FAR, 0, 0)
    mixer_pass(FAR, 1, 1)
    near_give(0)
    near_product(1)
    for m in range(FAR - 1, 0, -1):
        gift(m).wait_recv()
        for turn in range(2):
            for way in range(2):
                pass_on(m, 1 - way if turn == 0 else way, way)
        for turn in range(2):
            for way in range(2):
                mixer_pass(m, 1 - way if turn == 0 else way, way)
        if m == 3:
            near_return(0)
            near_give(1)
        elif m == 2:
            near_return(1)
    gift(0).wait_recv()

    def far_back(j):
        return put(
            r.far_ready.at[half(j)], r.far_got.at[half(j)],
            r.fback_sent.at[j], r.fback_here.at[j], **back(*far),
        )

    for j in range(2):
        chain(1, j, 0).wait_recv()
        chain(1, j, 1).wait_recv()
        r.far_ready[16 * j : 16 * j + 16] = (
            so_far(first_of(0), j)
            + chain_in[0, 0, j].astype(f32)
            + chain_in[1, 0, j].astype(f32)
        ).astype(bf16)
        far_back(j).start()

    mixer_publish()
    for i in range(NEAR):
        wait_near(near_back, stays_back, i)

    def near_sum(at):
        total = jnp.zeros((128, 512), f32)
        for n in range(2):
            got = r.near_got[4 * n : 4 * n + 4, :, at].reshape(128, 512)
            total = total + mm(r.back_high[n], got) + mm(r.back_low[n], got)
        r.summed[:, at] = total

    tiles(4, 512, near_sum)
    share_all(0)
    for j in range(2):
        far_back(j).wait()

    def far_sum(at):
        got = r.far_got[:, at]
        total = (
            r.summed[:, at]
            + mm(r.back_high[2, :, :SLOTS], got)
            + mm(r.back_low[2, :, :SLOTS], got)
        )
        r.part[1, :, :, at] = total.astype(bf16).reshape(NY, 16, 512)

    tiles(4, 512, far_sum)
    part_gift(1).start()
    scatter_all()
    publish_all()
    share_all(1)

    for j in range(2):
        for way in range(2):
            for k in range(reach(way, j)):
                ring(k, j, way).wait_send()
                relay(k, j, way).wait_send()
                chain(k + 1, j, way).wait_send()
                mixer_chain(k + 1, j, way).wait_send()
    for m in range(FAR + 1):
        gift(m).wait_send()
    near_gift(0).wait_send()
    near_gift(1).wait_send()
    for i in rounds:
        scatter(i).wait_send()
    for o in range(2):
        part_gift(o).wait_send()
        share(o, 0).wait()
        for i in rounds:
            publish(o, i).wait_send()
            share(o, i).wait()


def vm(*shape, dtype=jnp.bfloat16):
    return pltpu.VMEM(shape, dtype)


INPUTS = dict(
    mixer_in=ANY, mixer_gain=VM, w_value_in=ANY, w_gate_in=ANY, w_taps=VM,
    channel_gain=VM, w_output_in=ANY, expert_in=ANY, expert_gain=VM, routes=VM,
    scores=VM, gate_in=ANY, up_in=ANY, down_in=ANY,
)
F32 = jnp.float32
SCRATCH = dict(
    tokens_b=vm(128, 2048), tokens_a=vm(128, 2048), normed=vm(128, 2048), normed_a=vm(128, 2048),
    w_value=vm(96, 2048), w_gate=vm(96, 2048), weights=vm(2048, 256),
    down=vm(128, 2048), w_output=vm(96, 2048), pick=vm((NEAR + 1) * SLOTS, 128),
    back_high=vm(3, 128, 128), back_low=vm(3, 128, 128),
    far_send=vm(SLOTS, 2048), near_send=vm(NEAR, SLOTS, 2048),
    rows_far=vm(NY, 2, SLOTS, 2048), rows_near=vm(NEAR, 2, SLOTS, 2048),
    hidden_far=vm(NY, 2, SLOTS, 128), hidden_near=vm(NEAR, 2, SLOTS, 128),
    extended=vm(160, 128, dtype=F32), halo_out=vm(32, 128), halo_in=vm(32, 128),
    conv=vm(128, 96, dtype=F32), stats=vm(8, 128, dtype=F32),
    stats_pair=vm(8, 128, dtype=F32), stats_sum=vm(8, 128, dtype=F32),
    stats_all=vm(NY, 8, 128, dtype=F32), mine=vm(NY, SLOTS, 2048, dtype=F32),
    given=vm(NY, SLOTS, 2048), taken=vm(NY, SLOTS, 2048),
    chain_in=vm(2, FAR, 2, 16, 2048), chain_out=vm(2, FAR, 2, 16, 2048),
    near_given=vm(NEAR, SLOTS, 2048), near_taken=vm(NEAR, SLOTS, 2048),
    near_ready=vm(NEAR, SLOTS, 2048), near_got=vm(NEAR, SLOTS, 2048),
    far_ready=vm(SLOTS, 2048), far_got=vm(SLOTS, 2048), summed=vm(128, 2048, dtype=F32),
    part=vm(2, NY, 16, 2048), part_taken=vm(2, NY, 16, HALF), halves=vm(2, NY, 16, HALF),
    arrived=vm(NY, 16, HALF), mchain_in=vm(2, FAR, 2, 16, 512), mchain_out=vm(2, FAR, 2, 16, 512),
    load_sem=DMA((8,)), far_sent=DMA((2,)), far_here=DMA((2,)),
    near_sent=DMA((NEAR,)), near_here=DMA((NEAR,)), stay_sem=DMA((2,)),
    halo_sem=DMA((2,)), ring_sent=DMA((2, FAR, 2)), ring_here=DMA((2, FAR, 2)),
    relay_sent=DMA((2, FAR, 2)), relay_here=DMA((2, FAR, 2)), own_sent=DMA((2,)),
    own_here=DMA((2,)), nrelay_sent=DMA((NEAR,)), nrelay_here=DMA((NEAR,)),
    swap_sem=DMA((2,)), stats_sent=DMA((NY,)), stats_here=DMA((NY,)),
    gift_sent=DMA((NY,)), gift_here=DMA((NY,)), chain_sent=DMA((2, FAR, 2)),
    chain_here=DMA((2, FAR, 2)), ngift_sent=DMA((2,)), ngift_here=DMA((2,)),
    nback_sent=DMA((NEAR,)), nback_here=DMA((NEAR,)), fback_sent=DMA((2,)),
    fback_here=DMA((2,)), pgift_sent=DMA((2,)), pgift_here=DMA((2,)),
    scat_sent=DMA((NY,)), scat_here=DMA((NY,)), mchain_sent=DMA((2, FAR, 2)), mchain_here=DMA((2, FAR, 2)), pub_sent=DMA((2, NY)),
    pub_here=DMA((2, NY)), share_sent=DMA((2, NY)), share_here=DMA((2, NY)),
)
NAMES += list(INPUTS | dict(out_m=VM, out_e=VM) | SCRATCH)


def local(
    mixer_in,
    mixer_gain,
    w_value,
    w_gate,
    w_taps,
    channel_gain,
    w_output,
    expert_in,
    expert_gain,
    route_experts,
    route_scores,
    expert_gate,
    expert_up,
    expert_down,
):
    shape = (NY, 16, 2048)
    out_m, out_e = pl.pallas_call(
        whole_kernel,
        out_shape=(jax.ShapeDtypeStruct(shape, jnp.bfloat16),) * 2,
        in_specs=list(INPUTS.values()),
        out_specs=(VM, VM),
        scratch_shapes=list(SCRATCH.values()),
        compiler_params=pltpu.CompilerParams(
            collective_id=0, has_side_effects=True, vmem_limit_bytes=58 << 20
        ),
        name="whole",
    )(
        mixer_in, mixer_gain[None], w_value.T, w_gate.T, w_taps, channel_gain[None], w_output,
        expert_in, expert_gain[None], route_experts.T, route_scores.T,
        expert_gate, expert_up, expert_down,
    )
    return out_m.reshape(-1, 2048), out_e.reshape(-1, 2048)


def solution(mesh):
    split = Mesh(mesh.devices.reshape(NZ, NX, NY, 2), ("z", "x", "y", "c"))
    in_specs = (
        P(EP, None),
        P(),
        P(None, TP),
        P(None, TP),
        P(None, TP),
        P(TP),
        P(TP, None),
        P(EP, None),
        P(),
        P(EP, None),
        P(EP, None),
        P(EP, None, TP),
        P(EP, None, TP),
        P(EP, TP, None),
    )
    out_specs = (P(EP, None), P(EP, None))
    return jax.shard_map(local, mesh=split, in_specs=in_specs, out_specs=out_specs, check_vma=False)
```

```python
from types import SimpleNamespace

import jax
import jax.numpy as jnp
from jax import lax
from jax.experimental import pallas as pl
from jax.experimental.pallas import tpu as pltpu
from jax.sharding import Mesh
from jax.sharding import PartitionSpec as P

CONV_CH = 1536
CONV_W = 31
EP = ("z", "x")
TP = ("y", "c")
NZ, NX, NY = 8, 4, 8
SLOTS = 32
NEAR = 8
ITSELF = 4
HALF = 1024
FAR = NY // 2

epsilon = 1e-05
clamp_limit = 7.0
swish_slope = 1.702

VM = pl.BlockSpec(memory_space=pltpu.VMEM)
HBM = pl.BlockSpec(memory_space=pltpu.HBM)
DMA = pltpu.SemaphoreType.DMA


def far_shift(y, c):
    p = y // 4
    dz = (1 - p) * (3 + 2 * c) + p * (4 * (1 - c) + c * (6 - 4 * (y % 2)))
    return dz, y % 4


def near_shift(c, i):
    return (1, NZ - 1, 0, 2 + 4 * c)[i // 2], 2 * (i % 2) + c


def reach(way, j):
    return FAR if way == j else FAR - 1


def piece_of(ref, p):
    return ref.at[pl.ds(16 * (p // 2), 16), pl.ds(HALF * (p % 2), HALF)]


def put(src, dst, sent, landed, **device):
    return pltpu.make_async_remote_copy(
        src_ref=src,
        dst_ref=dst,
        send_sem=sent,
        recv_sem=landed,
        device_id=device,
        device_id_type=pl.DeviceIdType.MESH,
    )


def place():
    return tuple(lax.axis_index(a) for a in ("z", "x", "y", "c"))


def tiles(count, width, body):
    def step(n, _):
        body(pl.ds(pl.multiple_of(n * width, width), width))
        return 0

    lax.fori_loop(0, count, step, 0)


def mm(a, b):
    return jnp.dot(a, b, preferred_element_type=jnp.float32)


def norm_into(out, inputs, gain):
    def rows(at):
        widened = inputs[at, :].astype(jnp.float32)
        mean = jnp.mean(widened, axis=-1, keepdims=True)
        centred = widened - mean
        var = jnp.mean(jnp.square(centred), axis=-1, keepdims=True)
        out[at, :] = (centred * lax.rsqrt(var + epsilon) * gain[...]).astype(jnp.bfloat16)

    tiles(4, 32, rows)


NAMES = []


def whole_kernel(*refs):
    r = SimpleNamespace(**dict(zip(NAMES, refs)))
    z, x, y, c = place()
    other = 1 - c
    sides = ((y + 1) % NY, (y + NY - 1) % NY)
    block = z * NX + x
    after = (block + 1) % (NZ * NX)
    before = (block + NZ * NX - 1) % (NZ * NX)
    bf16, f32 = jnp.bfloat16, jnp.float32

    def on(dz, dx):
        return dict(z=(z + dz) % NZ, x=(x + dx) % NX)

    def back(dz, dx):
        return dict(z=(z + NZ - dz) % NZ, x=(x + NX - dx) % NX)

    far = far_shift(y, c)
    near = [near_shift(c, i) for i in range(NEAR)]
    itself = c == 0
    not_itself = c == 1

    load_sem = r.load_sem

    def load(n, src, dst):
        copy = pltpu.make_async_copy(src, dst, load_sem.at[n])
        copy.start()
        return copy

    load_routes = load(0, r.routes_in, r.routes)
    load_scores = load(1, r.scores_in, r.scores)
    load_tokens_b = load(2, r.expert_in, r.tokens_b)
    load_expert_gain = load(3, r.expert_gain_in, r.expert_gain)
    barrier = pltpu.get_barrier_semaphore()

    def greet(**device):
        pl.semaphore_signal(barrier, inc=1, device_id=device, device_id_type=pl.DeviceIdType.MESH)

    for n, shift in enumerate([far] + near):

        def both(shift=shift):
            greet(**on(*shift))
            greet(**back(*shift))

        if n == 1 + ITSELF:
            pl.when(not_itself)(both)
        else:
            both()
    greet(c=other)
    for i in range(1, NY):
        greet(y=(y + i) % NY)
    greet(z=after // NX, x=after % NX)
    greet(z=before // NX, x=before % NX)
    load_tokens_a = load(4, r.mixer_in, r.tokens_a)
    load_mixer_gain = load(5, r.mixer_gain_in, r.mixer_gain)
    load_w_value = load(6, r.w_value_in, r.w_value)
    load_w_gate = load(7, r.w_gate_in, r.w_gate)
    load_w_taps = load(8, r.w_taps_in, r.w_taps)
    load_gate = load(9, r.gate_in.at[0], r.weights.at[:, pl.ds(0, 128)])
    load_up = load(10, r.up_in.at[0], r.weights.at[:, pl.ds(128, 128)])
    load_down = load(11, r.down_in.at[0], r.down)
    load_channel_gain = load(12, r.channel_gain_in, r.channel_gain)
    load_w_output = load(13, r.w_output_in, r.w_output)

    load_routes.wait()
    load_scores.wait()
    routes = r.routes[...]
    raised = jnp.exp(r.scores[...])
    route_weights = raised / jnp.sum(raised, axis=0, keepdims=True)
    named, weight = [], []
    for shift in near + [far]:
        target = tuple(on(*shift).values())
        hit = routes == target[0] * NX + target[1]
        named.append(jnp.max(jnp.where(hit, 1.0, 0.0), axis=0, keepdims=True))
        weight.append(jnp.sum(jnp.where(hit, route_weights, 0.0), axis=0, keepdims=True))
    stacked = jnp.concatenate(named + [jnp.zeros((7, 128), f32)], axis=0).astype(bf16)
    sooner = lax.broadcasted_iota(jnp.int32, (128, 128), 0) < lax.broadcasted_iota(
        jnp.int32, (128, 128), 1
    )
    rank = mm(stacked, jnp.where(sooner, 1.0, 0.0).astype(bf16))
    slot = lax.broadcasted_iota(jnp.int32, (SLOTS, 128), 0).astype(f32)
    spread_weights = []
    for n in range(NEAR + 1):
        chosen = jnp.where(rank[n : n + 1] == slot, 1.0, 0.0) * named[n]
        r.pick[n * SLOTS : (n + 1) * SLOTS] = chosen.astype(bf16)
        spread_weights.append(chosen * weight[n])
    spread_weights.append(jnp.zeros((96, 128), f32))
    spread_weights = jnp.concatenate(spread_weights, axis=0)
    for n in range(3):
        turned = spread_weights[n * 128 : (n + 1) * 128].T
        high = turned.astype(bf16)
        r.back_high[n] = high
        r.back_low[n] = (turned - high.astype(f32)).astype(bf16)

    load_tokens_b.wait()
    load_expert_gain.wait()
    norm_into(r.normed, r.tokens_b, r.expert_gain)
    normed = r.normed

    def far_columns(at):
        r.far_send[:, at] = mm(r.pick[NEAR * SLOTS :], normed[:, at]).astype(bf16)

    tiles(4, 512, far_columns)
    pl.semaphore_wait(barrier, jnp.where(itself, 26, 28))

    rows_far, rows_near = r.rows_far, r.rows_near

    def far_out(p):
        return put(
            piece_of(r.far_send, p), piece_of(rows_far.at[y, c], p),
            r.far_sent.at[p], r.far_here.at[p], **on(*far),
        )

    for p in range(4):
        far_out(p).start()

    load_tokens_a.wait()
    load_mixer_gain.wait()
    norm_into(r.normed_a, r.tokens_a, r.mixer_gain)
    load_w_value.wait()
    load_w_gate.wait()

    def project(w):
        return lax.dot_general(
            r.normed_a[...], w[...], (((1,), (1,)), ((), ())), preferred_element_type=f32
        )

    values = project(r.w_value)
    gate_pre = project(r.w_gate)
    gated = (values * jax.nn.sigmoid(gate_pre)).astype(bf16)
    extended = r.extended
    extended[32:, :96] = gated.astype(f32)
    r.halo_out[...] = jnp.zeros((32, 128), bf16)
    r.halo_out[:, :96] = gated[96:]
    halo = put(
        r.halo_out, r.halo_in, r.halo_sem.at[0], r.halo_sem.at[1],
        z=after // NX, x=after % NX,
    )
    halo.start()

    def near_columns(at):
        r.near_send[:, :, at] = (
            mm(r.pick[: NEAR * SLOTS], normed[:, at]).astype(bf16).reshape(NEAR, SLOTS, 512)
        )

    tiles(4, 512, near_columns)

    def near_out(i):
        return put(
            r.near_send.at[i], rows_near.at[i, c],
            r.near_sent.at[i], r.near_here.at[i], **on(*near[i]),
        )

    stays_out = pltpu.make_async_copy(r.near_send.at[ITSELF], rows_near.at[ITSELF, c], r.stay_sem.at[0])

    def start_near(make, stay, i):
        if i == ITSELF:
            pl.when(itself)(lambda: stay.start())
            pl.when(not_itself)(lambda: make(i).start())
        else:
            make(i).start()

    def wait_near(make, stay, i):
        if i == ITSELF:
            pl.when(itself)(lambda: stay.wait())
            pl.when(not_itself)(lambda: make(i).wait())
        else:
            make(i).wait()

    for i in range(NEAR):
        start_near(near_out, stays_out, i)

    def origin(k, way):
        return (y + NY - k) % NY if way == 0 else (y + k) % NY

    def ring(k, p, way):
        piece = piece_of(rows_far.at[origin(k, way), c], p)
        return put(
            piece, piece, r.ring_sent.at[way, k, p], r.ring_here.at[way, k, p], y=sides[way]
        )

    def relay(k, p, way):
        piece = piece_of(rows_far.at[origin(k + 1, way), c], p)
        return put(
            piece, piece, r.relay_sent.at[way, k, p], r.relay_here.at[way, k, p], c=other
        )

    def own(p):
        piece = piece_of(rows_far.at[y, c], p)
        return put(piece, piece, r.own_sent.at[p], r.own_here.at[p], c=other)

    def near_relay(i):
        piece = rows_near.at[i, c]
        return put(piece, piece, r.nrelay_sent.at[i], r.nrelay_here.at[i], c=other)

    hidden_far, hidden_near = r.hidden_far, r.hidden_near

    def product(inputs):
        both = mm(inputs, r.weights[...])
        gate = jnp.minimum(both[:, :128], clamp_limit)
        up = jnp.clip(both[:, 128:], -clamp_limit, clamp_limit)
        return ((up + 1.0) * gate * jax.nn.sigmoid(swish_slope * gate)).astype(bf16)

    def far_product(sources):
        inputs = [rows_far[source].reshape(2 * SLOTS, 2048) for source in sources]
        outputs = product(jnp.concatenate(inputs, axis=0) if len(inputs) > 1 else inputs[0])
        for n, source in enumerate(sources):
            hidden_far[source] = outputs[n * 64 : n * 64 + 64].reshape(2, SLOTS, 128)

    def near_in(i):
        wait_near(near_out, stays_out, i)
        near_relay(i).start()

    def near_product(b):
        for i in range(4 * b, 4 * b + 4):
            near_relay(i).wait()
        at = pl.ds(4 * b, 4)
        hidden_near[at] = product(rows_near[at].reshape(8 * SLOTS, 2048)).reshape(4, 2, SLOTS, 128)

    def away(m, way):
        return (y + m) % NY if way == 0 else (y + NY - m) % NY

    mine, given, taken = r.mine, r.given, r.taken
    chain_in, chain_out = r.chain_in, r.chain_out

    def first_of(m):
        return 0 if m == FAR else 1 + 2 * (FAR - 1 - m)

    def gift(m):
        at = pl.ds(first_of(m), 1 if m in (0, FAR) else 2)
        return put(given.at[at], taken.at[at], r.gift_sent.at[m], r.gift_here.at[m], c=other)

    def partial(m):
        dests = [away(m, way) for way in range(1 if m in (0, FAR) else 2)]
        inputs = [hidden_far[dest, core] for core in (c, other) for dest in dests]
        inputs = jnp.concatenate(inputs, axis=0)
        count = len(dests)
        at_m = pl.ds(first_of(m), count)

        def cols(at):
            done = mm(inputs, r.down[:, at]).reshape(2, count, SLOTS, 512)
            mine[at_m, :, at] = done[0]
            given[at_m, :, at] = done[1].astype(bf16)

        tiles(4, 512, cols)
        gift(m).start()

    def chain(m, p, way):
        return put(
            piece_of(chain_out.at[way, m - 1], p), piece_of(chain_in.at[way, m - 1], p),
            r.chain_sent.at[way, m - 1, p], r.chain_here.at[way, m - 1, p], y=sides[way],
        )

    def span(p):
        return slice(16 * (p // 2), 16 * (p // 2) + 16), slice(HALF * (p % 2), HALF * (p % 2) + HALF)

    def so_far(i, p):
        rows, cols = span(p)
        return mine[i, rows, cols] + taken[i, rows, cols].astype(f32)

    def pass_on(m, p, way):
        rows, cols = span(p)
        total = so_far(first_of(m) + (0 if m == FAR else way), p)
        if m < reach(way, p // 2):
            chain(m + 1, p, way).wait_recv()
            total = total + chain_in[way, m, rows, cols].astype(f32)
        chain_out[way, m - 1, rows, cols] = total.astype(bf16)
        chain(m, p, way).start()

    def near_gift(b):
        at = pl.ds(4 * b, 4)
        return put(
            r.near_given.at[at], r.near_taken.at[at], r.ngift_sent.at[b], r.ngift_here.at[b], c=other
        )

    def near_give(b):
        blocks = pl.ds(4 * b, 4)
        inputs = hidden_near[blocks, other].reshape(4 * SLOTS, 128)

        def cols(at):
            done = mm(inputs, r.down[:, at]).astype(bf16)
            r.near_given[blocks, :, at] = done.reshape(4, SLOTS, 512)

        tiles(4, 512, cols)
        near_gift(b).start()

    def near_back(i):
        return put(
            r.near_ready.at[i], r.near_got.at[i],
            r.nback_sent.at[i], r.nback_here.at[i], **back(*near[i]),
        )

    stays_back = pltpu.make_async_copy(r.near_ready.at[ITSELF], r.near_got.at[ITSELF], r.stay_sem.at[1])

    def near_return(b):
        near_gift(b).wait_recv()
        blocks = pl.ds(4 * b, 4)
        inputs = hidden_near[blocks, c].reshape(4 * SLOTS, 128)

        def cols(at):
            done = mm(inputs, r.down[:, at])
            r.near_ready[blocks, :, at] = (
                done.reshape(4, SLOTS, 512) + r.near_taken[blocks, :, at].astype(f32)
            ).astype(bf16)

        tiles(4, 512, cols)
        for i in range(4 * b, 4 * b + 4):
            start_near(near_back, stays_back, i)

    mine_at = pl.ds(pl.multiple_of(c * HALF, HALF), HALF)
    their_at = pl.ds(pl.multiple_of(other * HALF, HALF), HALF)
    outs = (r.out_m, r.out_e)
    rounds = (4, 3, 5, 2, 6, 1, 7)

    def part_gift(o):
        return put(
            r.part.at[o, :, :, their_at], r.part_taken.at[o],
            r.pgift_sent.at[o], r.pgift_here.at[o], c=other,
        )

    def scatter(i):
        return put(
            r.halves.at[1, (y + i) % NY], r.arrived.at[y],
            r.scat_sent.at[i], r.scat_here.at[i], y=(y + i) % NY,
        )

    def scatter_all():
        part_gift(1).wait_recv()
        r.halves[1] = (
            r.part[1, :, :, mine_at].astype(f32) + r.part_taken[1].astype(f32)
        ).astype(bf16)
        for i in rounds:
            scatter(i).start()

    def publish(o, i):
        piece = outs[o].at[y, :, mine_at]
        return put(
            piece, piece, r.pub_sent.at[o, i], r.pub_here.at[o, i], y=(y + i) % NY
        )

    def share(o, i):
        piece = outs[o].at[(y + NY - i) % NY, :, mine_at]
        return put(piece, piece, r.share_sent.at[o, i], r.share_here.at[o, i], c=other)

    def publish_all():
        total = r.part[1, y, :, mine_at].astype(f32) + r.part_taken[1, y].astype(f32)
        for i in reversed(rounds):
            scatter(i).wait_recv()
            total = total + r.arrived[(y + NY - i) % NY].astype(f32)
        outs[1][y, :, mine_at] = total.astype(bf16)
        for i in rounds:
            publish(1, i).start()
        share(1, 0).start()

    def share_all(o):
        for i in reversed(rounds):
            publish(o, i).wait_recv()
            share(o, i).start()

    def mixer_part():
        load_w_output.wait()
        load_channel_gain.wait()
        total = r.stats_sum[...]
        for i in range(1, NY):
            stats_spread(i).wait()
            total = total + r.stats_all[(y + NY - i) % NY]
        turned = jnp.concatenate([total, jnp.zeros((120, 128), f32)], axis=0).T
        row_mean = turned[:, 0:1] / CONV_CH
        row_var = turned[:, 1:2] / CONV_CH - row_mean * row_mean
        scaled = (r.conv[...] - row_mean) * lax.rsqrt(row_var + epsilon)
        scaled = scaled * r.channel_gain[...]
        activated = (scaled * jax.nn.sigmoid(scaled)).astype(bf16)

        def cols(at):
            r.part[0, :, :, at] = (
                mm(activated, r.w_output[:, at]).astype(bf16).reshape(NY, 16, 512)
            )

        tiles(4, 512, cols)
        part_gift(0).start()

    def mixer_own(dest, j):
        at = slice(512 * j, 512 * j + 512)
        return r.halves[0, dest, :, at].astype(f32)

    def mixer_chain(m, j, way):
        return put(
            r.mchain_out.at[way, m - 1, j], r.mchain_in.at[way, m - 1, j],
            r.mchain_sent.at[way, m - 1, j], r.mchain_here.at[way, m - 1, j], y=sides[way],
        )

    def mixer_pass(m, j, way):
        total = mixer_own(away(m, way), j)
        if m < reach(way, j):
            mixer_chain(m + 1, j, way).wait_recv()
            total = total + r.mchain_in[way, m, j].astype(f32)
        r.mchain_out[way, m - 1, j] = total.astype(bf16)
        mixer_chain(m, j, way).start()

    def mixer_publish():
        for j in range(2):
            total = mixer_own(y, j)
            for way in range(2):
                mixer_chain(1, j, way).wait_recv()
                total = total + r.mchain_in[way, 0, j].astype(f32)
            r.out_m[y, :, pl.ds(pl.multiple_of(c * HALF + 512 * j, 512), 512)] = total.astype(bf16)
        for i in rounds:
            publish(0, i).start()
        share(0, 0).start()

    def conv_and_stats():
        halo.wait()
        load_w_taps.wait()
        keep = jnp.where(block == 0, 0.0, 1.0)
        extended[:32, :96] = r.halo_in[:, :96].astype(f32) * keep
        conv = jnp.zeros((128, 96), f32)
        for tap in range(CONV_W):
            conv = conv + extended[2 + tap : 130 + tap, :96] * r.w_taps[tap : tap + 1, :]
        r.conv[...] = conv
        lane = lax.broadcasted_iota(jnp.int32, (128, 128), 1)
        sums = jnp.sum(conv, axis=1, keepdims=True)
        squares = jnp.sum(conv * conv, axis=1, keepdims=True)
        columns = jnp.where(lane == 0, sums, jnp.where(lane == 1, squares, 0.0))
        r.stats[...] = columns.T[:8]
        stats_swap().start()

    def stats_spread(i):
        return put(
            r.stats_sum, r.stats_all.at[y], r.stats_sent.at[i], r.stats_here.at[i],
            y=(y + i) % NY,
        )

    def stats_swap():
        return put(r.stats, r.stats_pair, r.swap_sem.at[0], r.swap_sem.at[1], c=other)

    load_gate.wait()
    load_up.wait()
    load_down.wait()
    for p in range(4):
        far_out(p).wait()
        for way in range(2):
            ring(0, p, way).start()
        own(p).start()
    for k in range(FAR):
        for p in range(4):
            for way in range(2):
                if k < reach(way, p // 2):
                    ring(k, p, way).wait_recv()
                    if k + 1 < reach(way, p // 2):
                        ring(k + 1, p, way).start()
                    relay(k, p, way).start()
        if k == 0:
            for p in range(4):
                own(p).wait()
            far_product([y])
            conv_and_stats()
        elif k == 1:
            for i in range(4):
                near_in(i)
            stats_swap().wait()
            r.stats_sum[...] = r.stats[...] + r.stats_pair[...]
            for i in range(1, NY):
                stats_spread(i).start()
        elif k == 2:
            for i in range(4, NEAR):
                near_in(i)
            near_product(0)
            near_give(0)
        else:
            mixer_part()
        for p in range(4):
            for way in range(2):
                if k < reach(way, p // 2):
                    relay(k, p, way).wait_recv()
        far_product([origin(k + 1, way) for way in range(2 if k < FAR - 1 else 1)])
        partial(k + 1)

    gift(FAR).wait_recv()
    for p in range(4):
        pass_on(FAR, p, p // 2)
    part_gift(0).wait_recv()
    r.halves[0] = (
        r.part[0, :, :, mine_at].astype(f32) + r.part_taken[0].astype(f32)
    ).astype(bf16)
    mixer_pass(FAR, 0, 0)
    mixer_pass(FAR, 1, 1)
    near_return(0)
    near_product(1)
    near_give(1)
    for m in range(FAR - 1, 0, -1):
        gift(m).wait_recv()
        for turn in range(2):
            for q in range(2):
                for way in range(2):
                    pass_on(m, 2 * (1 - way if turn == 0 else way) + q, way)
        for turn in range(2):
            for way in range(2):
                mixer_pass(m, 1 - way if turn == 0 else way, way)
        if m == 3:
            near_return(1)
            partial(0)
    gift(0).wait_recv()

    def far_back(p):
        return put(
            piece_of(r.far_ready, p), piece_of(r.far_got, p),
            r.fback_sent.at[p], r.fback_here.at[p], **back(*far),
        )

    for p in range(4):
        rows, cols = span(p)
        chain(1, p, 0).wait_recv()
        chain(1, p, 1).wait_recv()
        r.far_ready[rows, cols] = (
            so_far(first_of(0), p)
            + chain_in[0, 0, rows, cols].astype(f32)
            + chain_in[1, 0, rows, cols].astype(f32)
        ).astype(bf16)
        far_back(p).start()

    mixer_publish()
    for i in range(NEAR):
        wait_near(near_back, stays_back, i)

    def near_sum(at):
        total = jnp.zeros((128, 512), f32)
        for n in range(2):
            got = r.near_got[4 * n : 4 * n + 4, :, at].reshape(128, 512)
            total = total + mm(r.back_high[n], got) + mm(r.back_low[n], got)
        r.summed[:, at] = total

    tiles(4, 512, near_sum)
    for p in range(4):
        far_back(p).wait()

    def far_sum(at):
        got = r.far_got[:, at]
        total = (
            r.summed[:, at]
            + mm(r.back_high[2, :, :SLOTS], got)
            + mm(r.back_low[2, :, :SLOTS], got)
        )
        r.part[1, :, :, at] = total.astype(bf16).reshape(NY, 16, 512)

    tiles(4, 512, far_sum)
    part_gift(1).start()
    scatter_all()
    share_all(0)
    publish_all()
    share_all(1)

    for p in range(4):
        for way in range(2):
            for k in range(reach(way, p // 2)):
                ring(k, p, way).wait_send()
                relay(k, p, way).wait_send()
                chain(k + 1, p, way).wait_send()
                if p % 2 == 0:
                    mixer_chain(k + 1, p // 2, way).wait_send()
    for m in range(FAR + 1):
        gift(m).wait_send()
    near_gift(0).wait_send()
    near_gift(1).wait_send()
    for i in rounds:
        scatter(i).wait_send()
    for o in range(2):
        part_gift(o).wait_send()
        share(o, 0).wait()
        for i in rounds:
            publish(o, i).wait_send()
            share(o, i).wait()


def vm(*shape, dtype=jnp.bfloat16):
    return pltpu.VMEM(shape, dtype)


INPUTS = dict(
    mixer_in=HBM, mixer_gain_in=HBM, w_value_in=HBM, w_gate_in=HBM, w_taps_in=HBM,
    channel_gain_in=HBM, w_output_in=HBM, expert_in=HBM, expert_gain_in=HBM, routes_in=HBM,
    scores_in=HBM, gate_in=HBM, up_in=HBM, down_in=HBM,
)
F32 = jnp.float32
SCRATCH = dict(
    mixer_gain=vm(1, 2048, dtype=F32), expert_gain=vm(1, 2048, dtype=F32),
    w_taps=vm(31, 96, dtype=F32), channel_gain=vm(1, 96, dtype=F32),
    routes=vm(4, 128, dtype=jnp.int32), scores=vm(4, 128, dtype=F32),
    tokens_b=vm(128, 2048), tokens_a=vm(128, 2048), normed=vm(128, 2048), normed_a=vm(128, 2048),
    w_value=vm(96, 2048), w_gate=vm(96, 2048), weights=vm(2048, 256),
    down=vm(128, 2048), w_output=vm(96, 2048), pick=vm((NEAR + 1) * SLOTS, 128),
    back_high=vm(3, 128, 128), back_low=vm(3, 128, 128),
    far_send=vm(SLOTS, 2048), near_send=vm(NEAR, SLOTS, 2048),
    rows_far=vm(NY, 2, SLOTS, 2048), rows_near=vm(NEAR, 2, SLOTS, 2048),
    hidden_far=vm(NY, 2, SLOTS, 128), hidden_near=vm(NEAR, 2, SLOTS, 128),
    extended=vm(160, 128, dtype=F32), halo_out=vm(32, 128), halo_in=vm(32, 128),
    conv=vm(128, 96, dtype=F32), stats=vm(8, 128, dtype=F32),
    stats_pair=vm(8, 128, dtype=F32), stats_sum=vm(8, 128, dtype=F32),
    stats_all=vm(NY, 8, 128, dtype=F32), mine=vm(NY, SLOTS, 2048, dtype=F32),
    given=vm(NY, SLOTS, 2048), taken=vm(NY, SLOTS, 2048),
    chain_in=vm(2, FAR, SLOTS, 2048), chain_out=vm(2, FAR, SLOTS, 2048),
    near_given=vm(NEAR, SLOTS, 2048), near_taken=vm(NEAR, SLOTS, 2048),
    near_ready=vm(NEAR, SLOTS, 2048), near_got=vm(NEAR, SLOTS, 2048),
    far_ready=vm(SLOTS, 2048), far_got=vm(SLOTS, 2048), summed=vm(128, 2048, dtype=F32),
    part=vm(2, NY, 16, 2048), part_taken=vm(2, NY, 16, HALF), halves=vm(2, NY, 16, HALF),
    arrived=vm(NY, 16, HALF), mchain_in=vm(2, FAR, 2, 16, 512), mchain_out=vm(2, FAR, 2, 16, 512),
    load_sem=DMA((14,)), far_sent=DMA((4,)), far_here=DMA((4,)),
    near_sent=DMA((NEAR,)), near_here=DMA((NEAR,)), stay_sem=DMA((2,)),
    halo_sem=DMA((2,)), ring_sent=DMA((2, FAR, 4)), ring_here=DMA((2, FAR, 4)),
    relay_sent=DMA((2, FAR, 4)), relay_here=DMA((2, FAR, 4)), own_sent=DMA((4,)),
    own_here=DMA((4,)), nrelay_sent=DMA((NEAR,)), nrelay_here=DMA((NEAR,)),
    swap_sem=DMA((2,)), stats_sent=DMA((NY,)), stats_here=DMA((NY,)),
    gift_sent=DMA((NY,)), gift_here=DMA((NY,)), chain_sent=DMA((2, FAR, 4)),
    chain_here=DMA((2, FAR, 4)), ngift_sent=DMA((2,)), ngift_here=DMA((2,)),
    nback_sent=DMA((NEAR,)), nback_here=DMA((NEAR,)), fback_sent=DMA((4,)),
    fback_here=DMA((4,)), pgift_sent=DMA((2,)), pgift_here=DMA((2,)),
    scat_sent=DMA((NY,)), scat_here=DMA((NY,)), mchain_sent=DMA((2, FAR, 2)), mchain_here=DMA((2, FAR, 2)), pub_sent=DMA((2, NY)),
    pub_here=DMA((2, NY)), share_sent=DMA((2, NY)), share_here=DMA((2, NY)),
)
NAMES += list(INPUTS | dict(out_m=VM, out_e=VM) | SCRATCH)


def local(
    mixer_in,
    mixer_gain,
    w_value,
    w_gate,
    w_taps,
    channel_gain,
    w_output,
    expert_in,
    expert_gain,
    route_experts,
    route_scores,
    expert_gate,
    expert_up,
    expert_down,
):
    shape = (NY, 16, 2048)
    out_m, out_e = pl.pallas_call(
        whole_kernel,
        out_shape=(jax.ShapeDtypeStruct(shape, jnp.bfloat16),) * 2,
        in_specs=list(INPUTS.values()),
        out_specs=(VM, VM),
        scratch_shapes=list(SCRATCH.values()),
        compiler_params=pltpu.CompilerParams(
            collective_id=0, has_side_effects=True, vmem_limit_bytes=58 << 20
        ),
        name="whole",
    )(
        mixer_in, mixer_gain[None], w_value.T, w_gate.T, w_taps, channel_gain[None], w_output,
        expert_in, expert_gain[None], route_experts.T, route_scores.T,
        expert_gate, expert_up, expert_down,
    )
    return out_m.reshape(-1, 2048), out_e.reshape(-1, 2048)


def solution(mesh):
    split = Mesh(mesh.devices.reshape(NZ, NX, NY, 2), ("z", "x", "y", "c"))
    in_specs = (
        P(EP, None),
        P(),
        P(None, TP),
        P(None, TP),
        P(None, TP),
        P(TP),
        P(TP, None),
        P(EP, None),
        P(),
        P(EP, None),
        P(EP, None),
        P(EP, None, TP),
        P(EP, None, TP),
        P(EP, TP, None),
    )
    out_specs = (P(EP, None), P(EP, None))
    return jax.shard_map(local, mesh=split, in_specs=in_specs, out_specs=out_specs, check_vma=False)
```
